512 devices in a mesh: sp: 64 (over z, y), tp: 8 (over x, core).
Axes of the slice: x: 4, y: 4, z: 16, core: 2. Of those that a mesh axis runs over, the one named last changes fastest.
Arguments:
- activations: bfloat16 [16384, 2048], P('sp', 'tp'), may hold values from -8 to 8
- norm_gain: float32 [2048], replicated, may hold values from 0.1 to 1.9
- win_query: bfloat16 [2048, 1024], P(None, 'tp'), may hold values from -1 to 1
- win_key: bfloat16 [2048, 512], P(None, 'tp'), may hold values from -1 to 1
- win_value: bfloat16 [2048, 512], P(None, 'tp'), may hold values from -0.125 to 0.125
- sink_logit: float32 [16], P('tp'), may hold values from 1 to 6
- lat_query: bfloat16 [2048, 1536], P(None, 'tp'), may hold values from -1 to 1
- key_value_down_weight: bfloat16 [2048, 128], replicated, may hold values from -0.125 to 0.125
- rope_key: bfloat16 [2048, 64], replicated, may hold values from -1 to 1
- latent_norm_gain: float32 [128], replicated, may hold values from 0.1 to 1.9
- key_up_weight: bfloat16 [128, 1024], P(None, 'tp'), may hold values from -0.5 to 0.5
- value_up_weight: bfloat16 [128, 1024], P(None, 'tp'), may hold values from -0.5 to 0.5
- out_win: bfloat16 [1024, 2048], P('tp'), may hold values from -0.359375 to 0.359375
- out_lat: bfloat16 [1024, 2048], P('tp'), may hold values from -0.59765625 to 0.59765625
Outputs:
- mixed: bfloat16 [16384, 2048], P('sp', 'tp')
The draws below stay inside these ranges and needn't reach their ends.
All inputs are finite; a program needn't handle non-finite values.
Results may differ from the reference program's by a relative error of at most 0.025.
Values may be sent and summed in bfloat16 or wider, within the bound.
A program may use at most 64 MiB of HBM per device.

```python
import jax
import jax.numpy as jnp
from jax import lax

MODEL_WIDTH = 2048
HEADS_A = 16
KV_A = 8
DH = 64
WINDOW = 128
LATENT_HEADS = 8
LATENT_WIDTH = 128
UNROTATED_WIDTH = 128
D_ROPE = 64
VALUE_WIDTH = 128
TOK_DEV = 256
SEQ = 16384


def drawn(key, row_count, col_count, spread):
    values = jnp.clip(jax.random.normal(key, (row_count, col_count), jnp.float32) * spread, -1.0, 1.0)
    return values.astype(jnp.bfloat16)


def draw_activations(key, part):
    key_base = jax.random.fold_in(key, 11)
    values = jnp.clip(jax.random.normal(key_base, (SEQ, MODEL_WIDTH), jnp.float32), -6.0, 6.0)
    return values.astype(jnp.bfloat16)


def draw_win_query(key, part):
    return drawn(jax.random.fold_in(key, 21), MODEL_WIDTH, HEADS_A * DH, MODEL_WIDTH ** (-0.5))


def draw_win_key(key, part):
    return drawn(jax.random.fold_in(key, 22), MODEL_WIDTH, KV_A * DH, MODEL_WIDTH ** (-0.5))


def draw_lat_query(key, part):
    return drawn(jax.random.fold_in(key, 23), MODEL_WIDTH, LATENT_HEADS * (UNROTATED_WIDTH + D_ROPE), 2.5 * MODEL_WIDTH ** (-0.5))


def draw_rope_key(key, part):
    return drawn(jax.random.fold_in(key, 24), MODEL_WIDTH, D_ROPE, MODEL_WIDTH ** (-0.5))


def levels(stream_key, shape, split, least, largest):
    gain, own = 1.0, jax.random.fold_in(stream_key, 6)
    for position, shards_of in split:
        heights = jnp.exp(jax.random.uniform(jax.random.fold_in(own, position), (shards_of,), jnp.float32, least / len(split), largest / len(split)))
        gain = gain * jnp.repeat(heights, shape[position] // shards_of).reshape([-1 if axis == position else 1 for axis in range(len(shape))])
    return gain


def bell_draw(own_key, dims, scale, bound, shards=(), kind=jnp.bfloat16):
    result = jax.random.normal(own_key, dims, jnp.float32) * scale
    if len(shards) > 0:
        result = levels(own_key, dims, shards, -0.22, 0.18) * result
    return jnp.clip(result, min=-bound, max=bound).astype(kind)


def setup_inputs(seed: int = 0) -> dict:
    key_of = jax.random.split(jax.random.key(seed), 15)
    return {
        "activations": draw_activations(jax.random.fold_in(key_of[14], 71), 0),
        "norm_gain": jnp.clip(1.0 + 0.18 * jax.random.normal(key_of[1], (MODEL_WIDTH,), jnp.float32), 0.1, 1.9),
        "win_query": draw_win_query(jax.random.fold_in(key_of[14], 71), 0),
        "win_key": draw_win_key(jax.random.fold_in(key_of[14], 71), 0),
        "win_value": bell_draw(key_of[4], (MODEL_WIDTH, KV_A * DH), MODEL_WIDTH ** -0.5, 0.125, ((1, 8),)),
        "sink_logit": jnp.clip(1.0 + 5.0 * jax.random.uniform(key_of[5], (HEADS_A,), jnp.float32) ** levels(key_of[5], (HEADS_A,), ((0, 8),), -0.2, 0.2), 1.0, 6.0),
        "lat_query": draw_lat_query(jax.random.fold_in(key_of[14], 71), 0),
        "key_value_down_weight": bell_draw(key_of[7], (MODEL_WIDTH, LATENT_WIDTH), MODEL_WIDTH ** -0.5, 0.125),
        "rope_key": draw_rope_key(jax.random.fold_in(key_of[14], 71), 0),
        "latent_norm_gain": jnp.clip(1.0 + 0.18 * jax.random.normal(key_of[9], (LATENT_WIDTH,), jnp.float32), 0.1, 1.9),
        "key_up_weight": bell_draw(key_of[10], (LATENT_WIDTH, LATENT_HEADS * UNROTATED_WIDTH), LATENT_WIDTH ** -0.5, 0.5, ((1, 8),)),
        "value_up_weight": bell_draw(key_of[11], (LATENT_WIDTH, LATENT_HEADS * VALUE_WIDTH), LATENT_WIDTH ** -0.5, 0.5, ((1, 8),)),
        "out_win": bell_draw(key_of[12], (HEADS_A * DH, MODEL_WIDTH), 0.06, 0.359375, ((0, 8),)),
        "out_lat": bell_draw(key_of[13], (LATENT_HEADS * VALUE_WIDTH, MODEL_WIDTH), 0.1, 0.59765625, ((0, 8),)),
    }


EPSILON = 1e-06
ROPE_BASE = 10000.0

def rotate(vectors, angles):
    half_width = vectors.shape[-1] // 2
    cosine_table = jnp.cos(angles)
    sine_table = jnp.sin(angles)
    lower_half = vectors[..., :half_width]
    upper_half = vectors[..., half_width:]
    return jnp.concatenate([lower_half * cosine_table - upper_half * sine_table, lower_half * sine_table + upper_half * cosine_table], axis=-1)

def rotary_angles(places, width):
    frequency = 1.0 / ROPE_BASE ** (jnp.arange(0, width, 2).astype(jnp.float32) / width)
    return places[:, None] * frequency[None, :]

def reference(activations, norm_gain, win_query, win_key, win_value, sink_logit, lat_query, key_value_down_weight, rope_key, latent_norm_gain, key_up_weight, value_up_weight, out_win, out_lat):
    widened = activations.astype(jnp.float32)
    row_scale = lax.rsqrt(lax.optimization_barrier(jnp.mean(widened * widened, axis=1)) + EPSILON)[:, None]
    normalized = (widened * norm_gain[None, :]).astype(jnp.bfloat16)

    def project(weight):
        return jnp.dot(normalized, weight, preferred_element_type=jnp.float32)
    win_queries = (project(win_query) * row_scale).astype(jnp.bfloat16)
    win_keys = (project(win_key) * row_scale).astype(jnp.bfloat16)
    win_values = (project(win_value) * row_scale).astype(jnp.bfloat16)
    places = jnp.arange(SEQ).astype(jnp.float32)
    angles = rotary_angles(places, D_ROPE)
    query_all = (project(lat_query) * row_scale).reshape(SEQ, LATENT_HEADS, UNROTATED_WIDTH + D_ROPE)
    query_plain = query_all[..., :UNROTATED_WIDTH].astype(jnp.bfloat16)
    query_turned = rotate(query_all[..., UNROTATED_WIDTH:], angles[:, None, :]).astype(jnp.bfloat16)
    compressed = project(key_value_down_weight)
    latent = (compressed * lax.rsqrt(lax.optimization_barrier(jnp.mean(compressed * compressed, axis=1, keepdims=True)) + EPSILON) * latent_norm_gain[None, :]).astype(jnp.bfloat16)
    key_rotary = rotate(project(rope_key) * row_scale, angles).astype(jnp.bfloat16)
    key_nope = jnp.dot(latent, key_up_weight, preferred_element_type=jnp.float32).astype(jnp.bfloat16)
    value_lat = jnp.dot(latent, value_up_weight, preferred_element_type=jnp.float32).astype(jnp.bfloat16)
    block_count = SEQ // WINDOW
    groups = HEADS_A // KV_A
    query_blocks = win_queries.reshape(block_count, WINDOW, KV_A, groups, DH)
    zero_rim = jnp.zeros((WINDOW, KV_A * DH), jnp.bfloat16)
    key_padded = jnp.concatenate([zero_rim, win_keys, zero_rim], 0).reshape(block_count + 2, WINDOW, KV_A, DH)
    value_padded = jnp.concatenate([zero_rim, win_values, zero_rim], 0).reshape(block_count + 2, WINDOW, KV_A, DH)
    key_near = jnp.concatenate([key_padded[:-2], key_padded[1:-1], key_padded[2:]], axis=1)
    value_near = jnp.concatenate([value_padded[:-2], value_padded[1:-1], value_padded[2:]], axis=1)
    slopes = jnp.exp2(-8.0 * jnp.arange(1, HEADS_A + 1).astype(jnp.float32) / HEADS_A).reshape(KV_A, groups)
    sink_table = sink_logit.reshape(KV_A, groups)

    def window_block(inputs):
        query_block, key_block, value_block, block_index = inputs
        query_pos = block_index * WINDOW + jnp.arange(WINDOW, dtype=jnp.int32)
        key_pos = (block_index - 1) * WINDOW + jnp.arange(3 * WINDOW, dtype=jnp.int32)
        distance = jnp.abs(query_pos[:, None] - key_pos[None, :])
        in_window = (distance <= WINDOW) & (key_pos[None, :] >= 0) & (key_pos[None, :] < SEQ)
        scores = jnp.einsum('qhgd,khd->hgqk', query_block.astype(jnp.float32), key_block.astype(jnp.float32)) * DH ** (-0.5)
        scores = scores - slopes[:, :, None, None] * distance.astype(jnp.float32)[None, None]
        scores = jnp.where(in_window[None, None], scores, -jnp.inf)
        row_peak = jnp.maximum(lax.optimization_barrier(jnp.max(scores, axis=3)), sink_table[:, :, None])
        weights = jnp.exp(scores - row_peak[..., None])
        denominator = lax.optimization_barrier(jnp.sum(weights, axis=3)) + jnp.exp(sink_table[:, :, None] - row_peak)
        rounded = lax.optimization_barrier(weights.astype(jnp.bfloat16)).astype(jnp.float32)
        blended = jnp.einsum('hgqk,khd->qhgd', rounded, value_block.astype(jnp.float32))
        blended = blended / jnp.transpose(denominator, (2, 0, 1))[..., None]
        return blended.reshape(WINDOW, HEADS_A * DH).astype(jnp.bfloat16)
    win_out = lax.map(window_block, (query_blocks, key_near, value_near, jnp.arange(block_count, dtype=jnp.int32))).reshape(SEQ, HEADS_A * DH)
    span_count = SEQ // TOK_DEV
    plain_keys = key_nope.astype(jnp.float32).reshape(SEQ, LATENT_HEADS, UNROTATED_WIDTH)
    lat_values = value_lat.astype(jnp.float32).reshape(SEQ, LATENT_HEADS, VALUE_WIDTH)
    turned_keys = key_rotary.astype(jnp.float32)

    def latent_block(inputs):
        plain_block, turned_block = inputs
        scores = (jnp.einsum('qhd,khd->hqk', plain_block.astype(jnp.float32), plain_keys) + jnp.einsum('qhd,kd->hqk', turned_block.astype(jnp.float32), turned_keys)) * (UNROTATED_WIDTH + D_ROPE) ** (-0.5)
        row_peak = lax.optimization_barrier(jnp.max(scores, axis=2, keepdims=True))
        weights = jnp.exp(scores - row_peak)
        totals = lax.optimization_barrier(jnp.sum(weights, axis=2))
        rounded = lax.optimization_barrier(weights.astype(jnp.bfloat16)).astype(jnp.float32)
        blended = jnp.einsum('hqk,khd->qhd', rounded, lat_values) / jnp.transpose(totals)[..., None]
        return blended.reshape(TOK_DEV, LATENT_HEADS * VALUE_WIDTH).astype(jnp.bfloat16)
    lat_out = lax.map(latent_block, (query_plain.reshape(span_count, TOK_DEV, LATENT_HEADS, UNROTATED_WIDTH), query_turned.reshape(span_count, TOK_DEV, LATENT_HEADS, D_ROPE))).reshape(SEQ, LATENT_HEADS * VALUE_WIDTH)
    summed = jnp.dot(win_out, out_win, preferred_element_type=jnp.float32) + jnp.dot(lat_out, out_lat, preferred_element_type=jnp.float32)
    return summed.astype(jnp.bfloat16)
```

```python
import functools

import jax
import jax.numpy as jnp
import numpy as np
from jax import lax
from jax.experimental import pallas as pl
from jax.experimental.pallas import tpu as pltpu
from jax.sharding import PartitionSpec as P

HEADS_A = 16
DH = 64
WINDOW = 128
PLAIN = 128
D_ROPE = 64
EPSILON = 1e-06
ROPE_BASE = 10000.0
NY = 4
REACH = 4
LOG2E = 1.4426950408889634
MESH = pl.DeviceIdType.MESH
BF16 = jnp.bfloat16
F32 = jnp.float32

NT = (((1,), (1,)), ((), ()))
TN = (((0,), (0,)), ((), ()))


def mm(a, b, dims=(((1,), (0,)), ((), ()))):
    return lax.dot_general(a, b, dims, preferred_element_type=F32)


def z_plan(nz):
    if nz == 4 * REACH:
        near = [REACH, -REACH]
        for k in range(1, REACH):
            near += [k, -k]
        return near, list(range(1, REACH + 1))[::-1], [-k for k in range(1, REACH)][::-1]
    half = nz // 2
    near = []
    for k in range(1, half + 1):
        near.append(k)
        if k != nz - k:
            near.append(-k)
    return near, [], []


def rotate(u, cos, sin):
    half = u.shape[1] // 2
    a, b = u[:, :half], u[:, half:]
    return jnp.concatenate([a * cos - b * sin, a * sin + b * cos], axis=1)


def kernel(
    cfg,
    act, gain, wq, wk, wv, sink, wlq, wkvd, wrope, lgain, kup, vup, ow, ol, ta, tb,
    out,
    actv, gv, lgv, tav, tbv, sinkv, wqv, wkv, wvv, wlqv, kdv, krv, kupv, vupv, wall,
    kps, kpr, xb, accq, acck, accv, accl, sqv,
    kbuf, qt, kvb, catt, cat, mst, lst, acc, pos, por, pls, plr, rss, rsr,
    lsem, wssem, wrsem, kpssem, kprsem, xssem, xrsem, kzs, kzr, kys, kyr, kds, kdr,
    qss, qrs, hss, hrs, pss, prs, lss, lrs, rs_s, rs_r,
):
    nz, ny, nx, tok, ft, model = cfg
    tp = 2 * nx
    ht = tok // 2
    sl = tok // tp
    s = lax.axis_index("sp")
    t = lax.axis_index("tp")
    sp = nz * ny
    z, y = s // ny, lax.rem(s, ny)
    x, c = t // 2, lax.rem(t, 2)
    other = 1 - c
    mate = t + 1 - 2 * c

    near, fwd_up, fwd_down = z_plan(nz)

    def at_z(dz):
        return lax.rem(z + dz + nz, nz)

    def at_y(dy):
        return lax.rem(y + dy + ny, ny)

    def rc(src, dst, ss, rs, sp_id, tp_id):
        return pltpu.make_async_remote_copy(
            src_ref=src, dst_ref=dst, send_sem=ss, recv_sem=rs,
            device_id=(sp_id, tp_id), device_id_type=MESH,
        )

    def done(ref, sem):
        pltpu.make_async_copy(ref, ref, sem).wait()

    rows = pl.ds(pl.multiple_of(t * ft, ft), ft)
    loads = [
        (act, actv), (gain, gv), (wkvd.at[rows], kdv), (wrope.at[rows], krv),
        (lgain, lgv), (ta, tav), (tb, tbv),
        (wq, wqv.at[c]), (wk, wkv.at[c]), (wv, wvv.at[c]), (wlq, wlqv.at[c]),
        (kup, kupv.at[c]), (vup, vupv.at[c]), (ow, wall.at[c]), (ol, wall.at[2 + c]),
    ]
    local = [pltpu.make_async_copy(a, b, lsem.at[i]) for i, (a, b) in enumerate(loads)]
    for copy in local:
        copy.start()

    own_sink = jnp.concatenate(
        [jnp.full((8, 128), sink[0], F32), jnp.full((8, 128), sink[1], F32)], axis=1
    )
    sinkv[c] = own_sink

    barrier = pltpu.get_barrier_semaphore()
    n_sig = 0

    def greet(sp_id, tp_id):
        pl.semaphore_signal(barrier, inc=1, device_id=(sp_id, tp_id), device_id_type=MESH)

    for d in range(1, tp):
        greet(s, lax.rem(t + d, tp))
        n_sig += 1
    for dz in near:
        greet(at_z(dz) * ny + y, t)
        n_sig += 1
    for dy in range(1, ny):
        greet(z * ny + at_y(dy), t)
        n_sig += 1
    side = lax.rem(s + 2 * c - 1 + sp, sp)
    greet(side, mate)
    n_sig += 1
    for i in range(4):
        local[i].wait()
    xn = actv[...].astype(F32)
    sq0 = jnp.sum(xn * xn, axis=1, keepdims=True)
    xn = (xn * gv[pl.ds(t, 1), :]).astype(BF16)
    kps[...] = jnp.concatenate(
        [mm(xn, kdv[...]), mm(xn, krv[...]), jnp.broadcast_to(sq0, (tok, D_ROPE))], axis=1
    ).reshape(tp, sl, 256)
    kpr[pl.ds(t, 1)] = kps[pl.ds(t, 1)]
    pl.semaphore_wait(barrier, n_sig)

    def order(d):
        hop = d // 2 + 1
        if nx == 4:
            hop = jnp.where(hop == 3, 3, 3 - hop)
        return jnp.where(d < tp - 2, lax.rem((x + hop) * 2 + lax.rem(c + d, 2), tp), mate)

    def send_kp(d, _):
        j = order(d)
        rc(kps.at[j], kpr.at[t], kpssem.at[d], kprsem.at[t], s, j).start()
        return 0

    lax.fori_loop(0, tp - 1, send_kp, 0)

    def send_x(d, _):
        j = order(d)
        half = pl.ds(pl.multiple_of(lax.rem(j, 2) * ht, ht), ht)
        rc(actv.at[half], xb.at[t], xssem.at[d], xrsem.at[t], s, j).start()
        return 0

    lax.fori_loop(0, tp - 1, send_x, 0)
    wsends = [
        (wq, wqv.at[c]), (wk, wkv.at[c]), (wv, wvv.at[c]), (wlq, wlqv.at[c]),
        (kup, kupv.at[c]), (vup, vupv.at[c]), (ow, wall.at[c]), (ol, wall.at[2 + c]),
        (sinkv.at[c], sinkv.at[c]),
    ]
    wdone = [
        wqv.at[other], wkv.at[other], wvv.at[other], wlqv.at[other], kupv.at[other],
        vupv.at[other], wall.at[other], wall.at[2 + other], sinkv.at[other],
    ]
    wcopies = [
        rc(a, b, wssem.at[i], wrsem.at[i], s, mate) for i, (a, b) in enumerate(wsends)
    ]
    for copy in wcopies:
        copy.start()

    for i in range(4, 7):
        local[i].wait()
    cos_a, sin_a = tav[pl.ds(s, 1), 0:32], tav[pl.ds(s, 1), 32:64]

    def angles(start, count):
        at = pl.ds(pl.multiple_of(start, count), count)
        cos_b, sin_b = tbv[at, 0:32], tbv[at, 32:64]
        return cos_a * cos_b - sin_a * sin_b, sin_a * cos_b + cos_a * sin_b

    def wait_kp(d, _):
        j = order(d)
        done(kpr.at[j], kprsem.at[j])
        return 0

    lax.fori_loop(0, tp - 1, wait_kp, 0)
    tot = kpr[0]
    for j in range(1, tp):
        tot = tot + kpr[j]
    comp, rope, sqs = tot[:, :128], tot[:, 128:192], tot[:, 192:193]
    lat = comp * lax.rsqrt(jnp.mean(comp * comp, axis=1, keepdims=True) + EPSILON) * lgv[...]
    kcos, ksin = angles(t * sl, sl)
    kro = rotate(rope * lax.rsqrt(sqs / model + EPSILON), kcos, ksin)
    chunk = jnp.concatenate(
        [lat, jnp.concatenate([kro[: sl // 2], kro[sl // 2 :]], axis=1)], axis=0
    ).astype(BF16)
    kbuf[z, c, y] = chunk

    def z_send(dz, zs, sem):
        rc(kbuf.at[zs, c, y], kbuf.at[zs, c, y], kzs.at[sem], kzr.at[zs],
           at_z(dz) * ny + y, t).start()

    for i, dz in enumerate(near):
        z_send(dz, z, i)

    def y_send(zs):
        for dy in range(1, ny):
            rc(kbuf.at[zs, c, y], kbuf.at[zs, c, y], kys.at[zs, dy - 1], kyr.at[zs],
               z * ny + at_y(dy), t).start()

    def step_a(dz):
        zs = at_z(dz)
        if not (isinstance(dz, int) and dz == 0):
            done(kbuf.at[zs, c, y], kzr.at[zs])
        y_send(zs)

    def step_b(dz):
        zs = at_z(dz)
        if ny > 1:
            done(kbuf.at[zs, c, pl.ds(0, ny - 1)], kyr.at[zs])
        rc(kbuf.at[zs, c], kbuf.at[zs, c], kds.at[zs], kdr.at[zs], s, mate).start()

    step_a(0)

    for i in range(7, 11):
        local[i].wait()
    for i in range(4):
        done(wdone[i], wrsem.at[i])

    def project(xk, k, first):
        xf = xk.astype(F32)
        sq = jnp.sum(xf * xf, axis=1, keepdims=True)
        xk = (xf * gv[pl.ds(k, 1), :]).astype(BF16)
        kr = pl.ds(pl.multiple_of(k * ft, ft), ft)
        for c2 in range(2):
            for a, w in ((accq, wqv), (acck, wkv), (accv, wvv), (accl, wlqv)):
                term = mm(xk, w[c2, kr, :])
                a[c2] = term if first else a[c2] + term
        sqv[...] = sq if first else sqv[...] + sq

    own_half = pl.ds(pl.multiple_of(c * ht, ht), ht)
    project(actv[own_half, :], t, True)

    def project_next(d, _):
        k = order(tp - 2 - d)
        done(xb.at[k], xrsem.at[k])
        project(xb[k], k, False)
        return 0

    lax.fori_loop(0, tp - 1, project_next, 0)

    scale = lax.rsqrt(sqv[...] / model + EPSILON)
    local[11].wait()
    done(wdone[4], wrsem.at[4])
    qcos, qsin = angles(c * ht, ht)
    factor = (PLAIN + D_ROPE) ** (-0.5) * LOG2E
    for c2 in range(2):
        ql = accl[c2] * scale
        plain = ql[:, :PLAIN].astype(BF16)
        qt[x, 0:128, c2 * ht : (c2 + 1) * ht] = (mm(kupv[c2], plain, NT) * factor).astype(BF16)
        turned = rotate(ql[:, PLAIN:], qcos, qsin) * factor
        qt[x, 128:192, c2 * ht : (c2 + 1) * ht] = jnp.transpose(turned).astype(BF16)
    for dx in range(1, nx):
        xo = lax.rem(x + dx, nx)
        rc(qt.at[x], qt.at[x], qss.at[dx - 1], qrs.at[x], s, xo * 2 + c).start()

    for c2 in range(2):
        kvb[1, c2, :, 0:64] = (acck[c2] * scale).astype(BF16)
        kvb[1, c2, :, 64:128] = (accv[c2] * scale).astype(BF16)
    to_mate = rc(kvb.at[1], kvb.at[2 * c], hss.at[0], hrs.at[2 * c], s, mate)
    to_mate.start()
    to_side = rc(kvb.at[1], kvb.at[2 * other], hss.at[1], hrs.at[2 * other], side, mate)
    to_side.start()

    if fwd_up:
        zs = at_z(-REACH)
        done(kbuf.at[zs, c, y], kzr.at[zs])
        for i, dz in enumerate(fwd_up):
            z_send(dz, zs, len(near) + i)
        y_send(zs)
        zs = at_z(REACH)
        done(kbuf.at[zs, c, y], kzr.at[zs])
        for i, dz in enumerate(fwd_down):
            z_send(dz, zs, len(near) + len(fwd_up) + i)
        y_send(zs)
        first = [dz for dz in near if abs(dz) != REACH]
        late = [-(REACH + k) for k in fwd_up[::-1]] + [REACH - k for k in fwd_down[::-1]]
        late.sort(key=abs)
        seen = [0] + first + [-REACH, REACH]
    else:
        first, late, seen = [-dz for dz in near], [], [0] + [-dz for dz in near]
    for dz in first:
        step_a(dz)
    for dz in seen:
        step_b(dz)

    for i in (0, 2):
        done(kvb.at[i], hrs.at[i])
    done(wdone[8], wrsem.at[8])
    kpos = lax.broadcasted_iota(jnp.int32, (3 * ht, ht), 0)
    qpos = lax.broadcasted_iota(jnp.int32, (3 * ht, ht), 1)
    apart = jnp.abs(qpos + ht - kpos)
    place = kpos + (s * 2 + c - 1) * ht
    inside = (apart <= WINDOW) & (place >= 0) & (place < sp * tok)
    apart = apart.astype(F32)
    for c2 in range(2):
        kw = kvb[:, c2, :, 0:64].reshape(3 * ht, DH)
        vw = kvb[:, c2, :, 64:128].reshape(3 * ht, DH)
        qw = (accq[c2] * scale).astype(BF16)
        for g in range(2):
            head = (x * 2 + c2) * 2 + g
            slope = jnp.exp2(
                jnp.full((1, ht), -8.0 / (2 * tp), F32) * (head + 1).astype(F32)
            )
            sc = mm(kw, qw[:, g * DH : (g + 1) * DH], NT) * DH ** (-0.5) - slope * apart
            sc = jnp.where(inside, sc, -jnp.inf)
            snk = sinkv[c2, 0:1, g * 128 : g * 128 + 128]
            peak = jnp.maximum(jnp.max(sc, axis=0, keepdims=True), snk)
            w = jnp.exp(sc - peak)
            den = jnp.sum(w, axis=0, keepdims=True) + jnp.exp(snk - peak)
            o = mm(vw, w.astype(BF16), TN) / den
            catt[(c2 * 2 + g) * DH : (c2 * 2 + g + 1) * DH, :] = o.astype(BF16)

    for dz in late:
        step_a(dz)
    for dz in late:
        step_b(dz)

    for dx in range(1, nx):
        xo = lax.rem(x + dx, nx)
        done(qt.at[xo], qrs.at[xo])
    mst[...] = jnp.full(mst.shape, -jnp.inf, F32)
    lst[...] = jnp.zeros(lst.shape, F32)
    acc[...] = jnp.zeros(acc.shape, F32)
    nkeys = 2 * ny * sl

    def batch(j, _):
        near_j = (j + 1) // 2
        dz = jnp.where(lax.rem(j, 2) == 0, near_j, -near_j)
        zs = lax.rem(z + dz + nz, nz)
        done(kbuf.at[zs, other], kdr.at[zs])
        both = kbuf[zs].reshape(2 * ny, sl + sl // 2, 128)
        latk = both[:, :sl, :].reshape(nkeys, 128)
        rp = both[:, sl:, :]
        rk = jnp.concatenate([rp[:, :, 0:64], rp[:, :, 64:128]], axis=1).reshape(nkeys, 64)
        keys = jnp.concatenate([latk, rk], axis=1)
        latt = jnp.transpose(latk)
        for xp in range(nx):
            sc = mm(keys, qt[xp])
            m_old = mst[xp]
            m_new = jnp.maximum(m_old, jnp.max(sc, axis=0, keepdims=True))
            alpha = jnp.exp2(m_old - m_new)
            p = jnp.exp2(sc - m_new)
            mst[xp] = m_new
            lst[xp] = lst[xp] * alpha + jnp.sum(p, axis=0, keepdims=True)
            acc[xp] = acc[xp] * alpha + mm(latt, p.astype(BF16))
        return 0

    lax.fori_loop(0, nz, batch, 0)

    for xp in range(nx):
        l = lst[xp]
        pos[xp] = (acc[xp] / l).astype(BF16)
        pls[xp] = jnp.broadcast_to(mst[xp] + jnp.log(l) * LOG2E, (8, 2 * ht))
    for dx in range(1, nx):
        xo = lax.rem(x + dx, nx)
        rc(pls.at[xo], plr.at[x], lss.at[dx - 1], lrs.at[x], s, xo * 2 + c).start()
        rc(pos.at[xo], por.at[x], pss.at[dx - 1], prs.at[x], s, xo * 2 + c).start()
    por[pl.ds(x, 1)] = pos[pl.ds(x, 1)]
    plr[pl.ds(x, 1)] = pls[pl.ds(x, 1)]
    for i in range(12, 15):
        local[i].wait()
    for i in range(5, 8):
        done(wdone[i], wrsem.at[i])
    for dx in range(1, nx):
        xo = lax.rem(x + dx, nx)
        done(plr.at[xo], lrs.at[xo])
        done(por.at[xo], prs.at[xo])
    lse = [plr[xp, 0:1, :] for xp in range(nx)]
    top = functools.reduce(jnp.maximum, lse)
    wts = [jnp.exp2(v - top) for v in lse]
    total = functools.reduce(lambda a, b: a + b, wts)
    mixed = por[0].astype(F32) * wts[0]
    for xp in range(1, nx):
        mixed = mixed + por[xp].astype(F32) * wts[xp]
    mixed = (mixed / total).astype(BF16)
    for h in range(2):
        catt[256 + h * 128 : 256 + (h + 1) * 128, :] = mm(
            vupv[h], mixed[:, h * ht : (h + 1) * ht], TN
        ).astype(BF16)
    cat[...] = jnp.transpose(catt[...])

    def out_block(d, _):
        j = order(d)
        cols = pl.ds(pl.multiple_of(j * ft, ft), ft)
        o = mm(cat[:, 0:128], wall[0, :, cols])
        for i in range(1, 4):
            o = o + mm(cat[:, i * 128 : (i + 1) * 128], wall[i, :, cols])
        rss[j] = o.astype(BF16)
        return j

    def send_block(d, _):
        j = out_block(d, _)
        rc(rss.at[j], rsr.at[x, c], rs_s.at[d], rs_r.at[x, c], s, j).start()
        return 0

    lax.fori_loop(0, tp - 1, send_block, 0)
    cols = pl.ds(pl.multiple_of(t * ft, ft), ft)
    o = mm(cat[:, 0:128], wall[0, :, cols])
    for i in range(1, 4):
        o = o + mm(cat[:, i * 128 : (i + 1) * 128], wall[i, :, cols])
    rsr[x, c] = o.astype(BF16)

    def wait_block(d, _):
        j = order(tp - 2 - d)
        jx, jc = j // 2, lax.rem(j, 2)
        done(rsr.at[jx, jc], rs_r.at[jx, jc])
        return 0

    lax.fori_loop(0, tp - 1, wait_block, 0)
    for c2 in range(2):
        total = rsr[0, c2].astype(F32)
        for xp in range(1, nx):
            total = total + rsr[xp, c2].astype(F32)
        out[c2 * ht : (c2 + 1) * ht, :] = total.astype(BF16)

    def sent(d, _):
        done(kps.at[0], kpssem.at[d])
        done(xb.at[0], xssem.at[d])
        done(rss.at[0], rs_s.at[d])
        return 0

    lax.fori_loop(0, tp - 1, sent, 0)
    for copy in wcopies:
        copy.wait_send()
    for i in range(len(near) + len(fwd_up) + len(fwd_down)):
        done(kbuf.at[0, 0, 0], kzs.at[i])

    def sent_keys(zs, _):
        for dy in range(ny - 1):
            done(kbuf.at[0, 0, 0], kys.at[zs, dy])
        done(kbuf.at[0, 0], kds.at[zs])
        return 0

    lax.fori_loop(0, nz, sent_keys, 0)
    for i in range(nx - 1):
        done(qt.at[0], qss.at[i])
        done(pls.at[0], lss.at[i])
        done(pos.at[0], pss.at[i])
    to_mate.wait_send()
    to_side.wait_send()


def tables(sp, tok):
    freq = 1.0 / ROPE_BASE ** (np.arange(0, D_ROPE, 2, dtype=np.float64) / D_ROPE)

    def table(places):
        angle = places[:, None] * freq[None, :]
        flat = np.concatenate([np.cos(angle), np.sin(angle)], axis=1)
        return np.pad(flat, ((0, 0), (0, 64))).astype(np.float32)

    return table(np.arange(sp) * float(tok)), table(np.arange(tok) * 1.0)


def per_device(nz, *args):
    (act, gain, wq, wk, wv, sink, wlq, wkvd, wrope, lgain, kup, vup, ow, ol) = args
    tp, sp = lax.axis_size("tp"), lax.axis_size("sp")
    nx = tp // 2
    ny = sp // nz
    tok, ft = act.shape
    model = tp * ft
    ht, sl = tok // 2, tok // tp
    ta, tb = tables(sp, tok)
    cfg = (nz, ny, nx, tok, ft, model)
    near, up, down = z_plan(nz)
    n_z = len(near) + len(up) + len(down)
    dma = pltpu.SemaphoreType.DMA
    v = pltpu.VMEM
    scratch = [
        v((tok, ft), BF16), v((tp, ft), F32), v((1, 128), F32), v((sp, 128), F32),
        v((tok, 128), F32), v((2, 8, 256), F32), v((2, model, 128), BF16),
        v((2, model, 64), BF16), v((2, model, 64), BF16), v((2, model, 192), BF16),
        v((ft, 128), BF16), v((ft, 64), BF16), v((2, 128, 128), BF16), v((2, 128, 128), BF16),
        v((4, 128, model), BF16),
        v((tp, sl, 256), F32), v((tp, sl, 256), F32), v((tp, ht, ft), BF16),
        v((2, ht, 128), F32), v((2, ht, 64), F32), v((2, ht, 64), F32), v((2, ht, 192), F32),
        v((ht, 1), F32),
        v((nz, 2, ny, sl + sl // 2, 128), BF16), v((nx, 192, 2 * ht), BF16),
        v((3, 2, ht, 128), BF16), v((512, ht), BF16), v((ht, 512), BF16),
        v((nx, 1, 2 * ht), F32), v((nx, 1, 2 * ht), F32), v((nx, 128, 2 * ht), F32),
        v((nx, 128, 2 * ht), BF16), v((nx, 128, 2 * ht), BF16),
        v((nx, 8, 2 * ht), F32), v((nx, 8, 2 * ht), F32),
        v((tp, ht, ft), BF16), v((nx, 2, ht, ft), BF16),
        dma((15,)), dma((9,)), dma((9,)), dma((tp,)), dma((tp,)), dma((tp,)), dma((tp,)),
        dma((n_z,)), dma((nz,)), dma((nz, max(ny - 1, 1))), dma((nz,)), dma((nz,)), dma((nz,)),
        dma((nx,)), dma((nx,)), dma((2,)), dma((3,)), dma((nx,)), dma((nx,)), dma((nx,)), dma((nx,)),
        dma((tp,)), dma((nx, 2)),
    ]
    hbm = pl.BlockSpec(memory_space=pl.ANY)
    specs = [hbm] * 16
    specs[5] = pl.BlockSpec(memory_space=pltpu.SMEM)
    return pl.pallas_call(
        functools.partial(kernel, cfg),
        out_shape=jax.ShapeDtypeStruct((tok, ft), BF16),
        in_specs=specs,
        out_specs=pl.BlockSpec(memory_space=pltpu.VMEM),
        scratch_shapes=scratch,
        compiler_params=pltpu.CompilerParams(
            collective_id=0, has_side_effects=True, vmem_limit_bytes=48 * 1024 * 1024
        ),
    )(
        act, gain.reshape(tp, ft), wq, wk, wv, sink, wlq, wkvd, wrope,
        lgain.reshape(1, 128), kup, vup, ow, ol, jnp.asarray(ta), jnp.asarray(tb),
    )


def solution(mesh):
    return jax.shard_map(
        functools.partial(per_device, mesh.shape["sp"] // NY),
        mesh=mesh,
        in_specs=(
            P("sp", "tp"), P(), P(None, "tp"), P(None, "tp"), P(None, "tp"), P("tp"),
            P(None, "tp"), P(), P(), P(), P(None, "tp"), P(None, "tp"), P("tp", None),
            P("tp", None),
        ),
        out_specs=P("sp", "tp"),
        check_vma=False,
    )
```

```python
import functools

import jax
import jax.numpy as jnp
import numpy as np
from jax import lax
from jax.experimental import pallas as pl
from jax.experimental.pallas import tpu as pltpu
from jax.sharding import PartitionSpec as P

HEADS_A = 16
DH = 64
WINDOW = 128
PLAIN = 128
D_ROPE = 64
EPSILON = 1e-06
ROPE_BASE = 10000.0
NY = 4
REACH = 4
LOG2E = 1.4426950408889634
MESH = pl.DeviceIdType.MESH
BF16 = jnp.bfloat16
F32 = jnp.float32

NT = (((1,), (1,)), ((), ()))
TN = (((0,), (0,)), ((), ()))


def mm(a, b, dims=(((1,), (0,)), ((), ()))):
    return lax.dot_general(a, b, dims, preferred_element_type=F32)


def z_plan(nz):
    if nz == 4 * REACH:
        near = [REACH, -REACH]
        for k in range(1, REACH):
            near += [k, -k]
        return near, list(range(1, REACH + 1))[::-1], [-k for k in range(1, REACH)][::-1]
    half = nz // 2
    near = []
    for k in range(1, half + 1):
        near.append(k)
        if k != nz - k:
            near.append(-k)
    return near, [], []


def rotate(u, cos, sin):
    half = u.shape[1] // 2
    a, b = u[:, :half], u[:, half:]
    return jnp.concatenate([a * cos - b * sin, a * sin + b * cos], axis=1)


def kernel(
    cfg,
    act, gain, wq, wk, wv, sink, wlq, wkvd, wrope, lgain, kup, vup, ow, ol, ta, tb,
    out,
    actv, gv, lgv, tav, tbv, sinkv, wqv, wtv, kdv, krv, kupv, vupv, wall,
    kps, kpr, xb, accq, acct, sqv,
    kbuf, qt, kvb, catt, cat, sco, latt, mst, pos, por, pls, plr, rss, rsr,
    lsem, wssem, wrsem, kpssem, kprsem, xssem, xrsem, kzs, kzr, kys, kyr, kds, kdr,
    qss, qrs, hss, hrs, pss, prs, lss, lrs, rs_s, rs_r,
):
    nz, ny, nx, tok, ft, model = cfg
    tp = 2 * nx
    ht = tok // 2
    sl = tok // tp
    s = lax.axis_index("sp")
    t = lax.axis_index("tp")
    sp = nz * ny
    z, y = s // ny, lax.rem(s, ny)
    x, c = t // 2, lax.rem(t, 2)
    other = 1 - c
    mate = t + 1 - 2 * c

    near, fwd_up, fwd_down = z_plan(nz)
    n_seen = 2 * REACH + 1 if fwd_up else nz
    mine = pl.ds(pl.multiple_of(c * 128, 128), 128)
    mine_lat = pl.ds(pl.multiple_of((2 + c) * 128, 128), 128)
    theirs = pl.ds(pl.multiple_of(other * 128, 128), 128)
    theirs_lat = pl.ds(pl.multiple_of((2 + other) * 128, 128), 128)

    def at_z(dz):
        return lax.rem(z + dz + nz, nz)

    def at_y(dy):
        return lax.rem(y + dy + ny, ny)

    def rc(src, dst, ss, rs, sp_id, tp_id):
        return pltpu.make_async_remote_copy(
            src_ref=src, dst_ref=dst, send_sem=ss, recv_sem=rs,
            device_id=(sp_id, tp_id), device_id_type=MESH,
        )

    def done(ref, sem):
        pltpu.make_async_copy(ref, ref, sem).wait()

    barrier = pltpu.get_barrier_semaphore()
    n_sig = 0

    def greet(sp_id, tp_id):
        pl.semaphore_signal(barrier, inc=1, device_id=(sp_id, tp_id), device_id_type=MESH)

    for d in range(1, tp):
        greet(s, lax.rem(t + d, tp))
        n_sig += 1
    for dz in near:
        greet(at_z(dz) * ny + y, t)
        n_sig += 1
    for dy in range(1, ny):
        greet(z * ny + at_y(dy), t)
        n_sig += 1
    side = lax.rem(s + 2 * c - 1 + sp, sp)
    greet(side, mate)
    n_sig += 1
    rows = pl.ds(pl.multiple_of(t * ft, ft), ft)
    loads = [
        (act, actv), (wkvd.at[rows], kdv), (wrope.at[:, rows], krv),
    ] + [(gain.at[pl.ds(k * ft, ft)], gv.at[k]) for k in range(tp)] + [
        (lgain, lgv), (ta, tav), (tb, tbv),
        (wq, wqv.at[c]), (wk, wtv.at[c, 0:64]), (wv, wtv.at[c, 64:128]),
        (wlq, wtv.at[c, 128:320]),
        (kup, kupv.at[c]), (vup, vupv.at[c]), (ow, wall.at[mine]), (ol, wall.at[mine_lat]),
    ]
    local = [pltpu.make_async_copy(a, b, lsem.at[i]) for i, (a, b) in enumerate(loads)]
    early = 3 + tp
    for copy in local[:early]:
        copy.start()

    own_sink = jnp.concatenate(
        [jnp.full((8, 128), sink[0], F32), jnp.full((8, 128), sink[1], F32)], axis=1
    )
    sinkv[c] = own_sink

    for copy in local[:early]:
        copy.wait()
    xn = actv[...].astype(F32)
    sq0 = jnp.sum(xn * xn, axis=1, keepdims=True)
    xn = (xn * gv[pl.ds(t, 1), :]).astype(BF16)
    kps[...] = jnp.concatenate(
        [mm(xn, kdv[...]), mm(xn, krv[...], NT), jnp.broadcast_to(sq0, (tok, D_ROPE))],
        axis=1,
    ).astype(BF16).reshape(tp, sl, 256)
    kpr[pl.ds(t, 1)] = kps[pl.ds(t, 1)]
    pl.semaphore_wait(barrier, n_sig)

    def order(d):
        hop = d // 2 + 1
        if nx == 4:
            hop = jnp.where(hop == 3, 3, 3 - hop)
        return jnp.where(d < tp - 2, lax.rem((x + hop) * 2 + lax.rem(c + d, 2), tp), mate)

    def send_kp(d, _):
        j = order(d)
        rc(kps.at[j], kpr.at[t], kpssem.at[d], kprsem.at[t], s, j).start()
        return 0

    lax.fori_loop(0, tp - 1, send_kp, 0)

    def send_x(d, _):
        j = order(d)
        half = pl.ds(pl.multiple_of(lax.rem(j, 2) * ht, ht), ht)
        rc(actv.at[half], xb.at[t], xssem.at[d], xrsem.at[t], s, j).start()
        return 0

    lax.fori_loop(0, tp - 1, send_x, 0)
    for copy in local[early:]:
        copy.start()
    wsends = [
        (wq, wqv.at[c]), (wk, wtv.at[c, 0:64]), (wv, wtv.at[c, 64:128]),
        (wlq, wtv.at[c, 128:320]), (kup, kupv.at[c]), (vup, vupv.at[c]),
        (ow, wall.at[mine]), (ol, wall.at[mine_lat]), (sinkv.at[c], sinkv.at[c]),
    ]
    wdone = [
        wqv.at[other], wtv.at[other, 0:64], wtv.at[other, 64:128], wtv.at[other, 128:320],
        kupv.at[other], vupv.at[other], wall.at[theirs], wall.at[theirs_lat], sinkv.at[other],
    ]
    wcopies = [
        rc(a, b, wssem.at[i], wrsem.at[i], s, mate) for i, (a, b) in enumerate(wsends)
    ]
    for copy in wcopies:
        copy.start()

    for copy in local[early : early + 3]:
        copy.wait()
    cos_a, sin_a = tav[pl.ds(s, 1), 0:32], tav[pl.ds(s, 1), 32:64]

    def angles(start, count):
        at = pl.ds(pl.multiple_of(start, count), count)
        cos_b, sin_b = tbv[at, 0:32], tbv[at, 32:64]
        return cos_a * cos_b - sin_a * sin_b, sin_a * cos_b + cos_a * sin_b

    def wait_kp(d, _):
        j = order(d)
        done(kpr.at[j], kprsem.at[j])
        return 0

    lax.fori_loop(0, tp - 1, wait_kp, 0)
    tot = kpr[0].astype(F32)
    for j in range(1, tp):
        tot = tot + kpr[j].astype(F32)
    comp, rope, sqs = tot[:, :128], tot[:, 128:192], tot[:, 192:193]
    lat = comp * lax.rsqrt(jnp.mean(comp * comp, axis=1, keepdims=True) + EPSILON) * lgv[...]
    kcos, ksin = angles(t * sl, sl)
    kro = rotate(rope * lax.rsqrt(sqs / model + EPSILON), kcos, ksin)
    chunk = jnp.concatenate(
        [lat, jnp.concatenate([kro[: sl // 2], kro[sl // 2 :]], axis=1)], axis=0
    ).astype(BF16)
    kbuf[z, c, y] = chunk

    def z_send(dz, zs, sem):
        rc(kbuf.at[zs, c, y], kbuf.at[zs, c, y], kzs.at[sem], kzr.at[zs],
           at_z(dz) * ny + y, t).start()

    for i, dz in enumerate(near):
        z_send(dz, z, i)

    def y_send(zs):
        for dy in range(1, ny):
            rc(kbuf.at[zs, c, y], kbuf.at[zs, c, y], kys.at[zs, dy - 1], kyr.at[zs],
               z * ny + at_y(dy), t).start()

    def zs_of(j):
        far = (j + 1) // 2
        return lax.rem(z + jnp.where(lax.rem(j, 2) == 0, far, nz - far), nz)

    def step_a(j, _):
        zs = zs_of(j)
        done(kbuf.at[zs, c, y], kzr.at[zs])
        y_send(zs)
        return 0

    def step_b(j, _):
        zs = zs_of(j)
        if ny > 1:
            done(kbuf.at[zs, c, pl.ds(0, ny - 1)], kyr.at[zs])
        rc(kbuf.at[zs, c], kbuf.at[zs, c], kds.at[zs], kdr.at[zs], s, mate).start()
        return 0

    y_send(z)

    for copy in local[early + 3 : early + 7]:
        copy.wait()
    for i in range(4):
        done(wdone[i], wrsem.at[i])

    def project(xk, k, first):
        xf = xk.astype(F32)
        sq = jnp.sum(xf * xf, axis=1, keepdims=True)
        xk = (xf * gv[pl.ds(k, 1), :]).astype(BF16)
        kr = pl.ds(pl.multiple_of(k * ft, ft), ft)
        for c2 in range(2):
            term = mm(xk, wqv[c2, kr, :])
            accq[c2] = term if first else accq[c2] + term
            term = mm(xk, wtv[c2, :, kr], NT)
            acct[c2] = term if first else acct[c2] + term
        sqv[...] = sq if first else sqv[...] + sq

    own_half = pl.ds(pl.multiple_of(c * ht, ht), ht)
    project(actv[own_half, :], t, True)

    def project_next(d, _):
        k = order(tp - 2 - d)
        done(xb.at[k], xrsem.at[k])
        project(xb[k], k, False)
        return 0

    lax.fori_loop(0, tp - 3, project_next, 0)

    if fwd_up:
        lax.fori_loop(1, 2 * REACH - 1, step_a, 0)
        zs = at_z(-REACH)
        done(kbuf.at[zs, c, y], kzr.at[zs])
        for i, dz in enumerate(fwd_up):
            z_send(dz, zs, len(near) + i)
        y_send(zs)
        zs = at_z(REACH)
        done(kbuf.at[zs, c, y], kzr.at[zs])
        for i, dz in enumerate(fwd_down):
            z_send(dz, zs, len(near) + len(fwd_up) + i)
        y_send(zs)
    else:
        lax.fori_loop(1, nz, step_a, 0)
    lax.fori_loop(max(tp - 3, 0), tp - 1, project_next, 0)

    scale = lax.rsqrt(sqv[...] / model + EPSILON)
    local[early + 7].wait()
    done(wdone[4], wrsem.at[4])
    qcos, qsin = angles(c * ht, ht)
    factor = (PLAIN + D_ROPE) ** (-0.5) * LOG2E
    for c2 in range(2):
        ql = acct[c2, :, 128:320] * scale
        plain = ql[:, :PLAIN].astype(BF16)
        qt[x, 0:128, c2 * ht : (c2 + 1) * ht] = (mm(kupv[c2], plain, NT) * factor).astype(BF16)
        turned = rotate(ql[:, PLAIN:], qcos, qsin) * factor
        qt[x, 128:192, c2 * ht : (c2 + 1) * ht] = jnp.transpose(turned).astype(BF16)
    for dx in range(1, nx):
        xo = lax.rem(x + dx, nx)
        rc(qt.at[x], qt.at[x], qss.at[dx - 1], qrs.at[x], s, xo * 2 + c).start()

    for c2 in range(2):
        kvb[1, c2] = (acct[c2, :, 0:128] * scale).astype(BF16)
    to_mate = rc(kvb.at[1], kvb.at[2 * c], hss.at[0], hrs.at[2 * c], s, mate)
    to_mate.start()
    to_side = rc(kvb.at[1], kvb.at[2 * other], hss.at[1], hrs.at[2 * other], side, mate)
    to_side.start()

    early_b = min(5, n_seen)
    lax.fori_loop(0, early_b, step_b, 0)
    lax.fori_loop(n_seen, nz, step_a, 0)
    lax.fori_loop(early_b, n_seen, step_b, 0)

    for i in (0, 2):
        done(kvb.at[i], hrs.at[i])
    done(wdone[8], wrsem.at[8])
    kpos = lax.broadcasted_iota(jnp.int32, (3 * ht, ht), 0)
    qpos = lax.broadcasted_iota(jnp.int32, (3 * ht, ht), 1)
    apart = jnp.abs(qpos + ht - kpos)
    place = kpos + (s * 2 + c - 1) * ht
    inside = (apart <= WINDOW) & (place >= 0) & (place < sp * tok)
    apart = apart.astype(F32)
    for c2 in range(2):
        kw = kvb[:, c2, :, 0:64].reshape(3 * ht, DH)
        vw = kvb[:, c2, :, 64:128].reshape(3 * ht, DH)
        qw = (accq[c2] * scale).astype(BF16)
        for g in range(2):
            head = (x * 2 + c2) * 2 + g
            slope = jnp.exp2(
                jnp.full((1, ht), -8.0 / (2 * tp), F32) * (head + 1).astype(F32)
            )
            sc = mm(kw, qw[:, g * DH : (g + 1) * DH], NT) * DH ** (-0.5) - slope * apart
            sc = jnp.where(inside, sc, -jnp.inf)
            snk = sinkv[c2, 0:1, g * 128 : g * 128 + 128]
            peak = jnp.maximum(jnp.max(sc, axis=0, keepdims=True), snk)
            w = jnp.exp(sc - peak)
            den = jnp.sum(w, axis=0, keepdims=True) + jnp.exp(snk - peak)
            o = mm(vw, w.astype(BF16), TN) / den
            catt[(c2 * 2 + g) * DH : (c2 * 2 + g + 1) * DH, :] = o.astype(BF16)

    for dx in range(1, nx):
        xo = lax.rem(x + dx, nx)
        done(qt.at[xo], qrs.at[xo])
    mst[...] = jnp.full(mst.shape, -jnp.inf, F32)
    nkeys = 2 * ny * sl
    keys_all = nz * nkeys

    def step_c(j, _):
        zs = zs_of(j)
        done(kbuf.at[zs, other], kdr.at[zs])
        both = kbuf[zs].reshape(2 * ny, sl + sl // 2, 128)
        latk = both[:, :sl, :].reshape(nkeys, 128)
        rp = both[:, sl:, :]
        rk = jnp.concatenate([rp[:, :, 0:64], rp[:, :, 64:128]], axis=1).reshape(nkeys, 64)
        keys = jnp.concatenate([latk, rk], axis=1)
        at = pl.ds(pl.multiple_of(zs * nkeys, nkeys), nkeys)
        latt[:, at] = jnp.transpose(latk)
        for xp in range(nx):
            sc = mm(keys, qt[xp])
            sco[xp, at, :] = sc
            mst[xp] = jnp.maximum(mst[xp], jnp.max(sc.reshape(nkeys // 8, 8, 2 * ht), axis=0))
        return 0

    def step_cb(i, _):
        step_c(i, 0)
        step_b(n_seen + i, 0)
        return 0

    lax.fori_loop(0, nz - n_seen, step_cb, 0)
    lax.fori_loop(nz - n_seen, nz, step_c, 0)

    part = min(1024, keys_all)

    def weigh(xp):
        peak = jnp.max(mst[xp], axis=0, keepdims=True)
        l8 = jnp.zeros((8, 2 * ht), F32)
        o = jnp.zeros((128, 2 * ht), F32)
        for k in range(keys_all // part):
            p = jnp.exp2(sco[xp, k * part : (k + 1) * part, :] - peak)
            l8 = l8 + jnp.sum(p.reshape(part // 8, 8, 2 * ht), axis=0)
            o = o + mm(latt[:, k * part : (k + 1) * part], p.astype(BF16))
        l = jnp.sum(l8, axis=0, keepdims=True)
        pos[xp] = (o / l).astype(BF16)
        pls[xp] = jnp.broadcast_to(peak + jnp.log(l) * LOG2E, (8, 2 * ht))

    def weigh_next(i, _):
        dx = i + 1
        if nx == 4:
            dx = jnp.where(dx == 3, 3, 3 - dx)
        xo = lax.rem(x + dx, nx)
        weigh(xo)
        rc(pls.at[xo], plr.at[x], lss.at[i], lrs.at[x], s, xo * 2 + c).start()
        rc(pos.at[xo], por.at[x], pss.at[i], prs.at[x], s, xo * 2 + c).start()
        return 0

    lax.fori_loop(0, nx - 1, weigh_next, 0)
    weigh(x)
    por[pl.ds(x, 1)] = pos[pl.ds(x, 1)]
    plr[pl.ds(x, 1)] = pls[pl.ds(x, 1)]
    for copy in local[early + 8 :]:
        copy.wait()
    for i in range(5, 8):
        done(wdone[i], wrsem.at[i])
    for dx in range(1, nx):
        xo = lax.rem(x + dx, nx)
        done(plr.at[xo], lrs.at[xo])
        done(por.at[xo], prs.at[xo])
    lse = [plr[xp, 0:1, :] for xp in range(nx)]
    top = functools.reduce(jnp.maximum, lse)
    wts = [jnp.exp2(v - top) for v in lse]
    total = functools.reduce(lambda a, b: a + b, wts)
    mixed = por[0].astype(F32) * wts[0]
    for xp in range(1, nx):
        mixed = mixed + por[xp].astype(F32) * wts[xp]
    mixed = (mixed / total).astype(BF16)
    for h in range(2):
        catt[256 + h * 128 : 256 + (h + 1) * 128, :] = mm(
            vupv[h], mixed[:, h * ht : (h + 1) * ht], TN
        ).astype(BF16)
    cat[...] = jnp.transpose(catt[...])

    def out_block(j):
        cols = pl.ds(pl.multiple_of(j * ft, ft), ft)
        return mm(cat[...], wall[:, cols]).astype(BF16)

    def send_block(d, _):
        j = order(d)
        rss[j] = out_block(j)
        rc(rss.at[j], rsr.at[x, c], rs_s.at[d], rs_r.at[x, c], s, j).start()
        return 0

    lax.fori_loop(0, tp - 1, send_block, 0)
    rsr[x, c] = out_block(t)

    def wait_block(d, _):
        j = order(tp - 2 - d)
        jx, jc = j // 2, lax.rem(j, 2)
        done(rsr.at[jx, jc], rs_r.at[jx, jc])
        return 0

    lax.fori_loop(0, tp - 1, wait_block, 0)
    for c2 in range(2):
        total = rsr[0, c2].astype(F32)
        for xp in range(1, nx):
            total = total + rsr[xp, c2].astype(F32)
        out[c2 * ht : (c2 + 1) * ht, :] = total.astype(BF16)

    def sent(d, _):
        done(kps.at[0], kpssem.at[d])
        done(xb.at[0], xssem.at[d])
        done(rss.at[0], rs_s.at[d])
        return 0

    lax.fori_loop(0, tp - 1, sent, 0)
    for copy in wcopies:
        copy.wait_send()
    for i in range(len(near) + len(fwd_up) + len(fwd_down)):
        done(kbuf.at[0, 0, 0], kzs.at[i])

    def sent_keys(zs, _):
        for dy in range(ny - 1):
            done(kbuf.at[0, 0, 0], kys.at[zs, dy])
        done(kbuf.at[0, 0], kds.at[zs])
        return 0

    lax.fori_loop(0, nz, sent_keys, 0)
    for i in range(nx - 1):
        done(qt.at[0], qss.at[i])
        done(pls.at[0], lss.at[i])
        done(pos.at[0], pss.at[i])
    to_mate.wait_send()
    to_side.wait_send()


def tables(sp, tok):
    freq = 1.0 / ROPE_BASE ** (np.arange(0, D_ROPE, 2, dtype=np.float64) / D_ROPE)

    def table(places):
        angle = places[:, None] * freq[None, :]
        flat = np.concatenate([np.cos(angle), np.sin(angle)], axis=1)
        return np.pad(flat, ((0, 0), (0, 64))).astype(np.float32)

    return table(np.arange(sp) * float(tok)), table(np.arange(tok) * 1.0)


def per_device(nz, *args):
    (act, gain, wq, wk, wv, sink, wlq, wkvd, wrope, lgain, kup, vup, ow, ol) = args
    tp, sp = lax.axis_size("tp"), lax.axis_size("sp")
    nx = tp // 2
    ny = sp // nz
    tok, ft = act.shape
    model = tp * ft
    ht, sl = tok // 2, tok // tp
    ta, tb = tables(sp, tok)
    cfg = (nz, ny, nx, tok, ft, model)
    near, up, down = z_plan(nz)
    n_z = len(near) + len(up) + len(down)
    dma = pltpu.SemaphoreType.DMA
    v = pltpu.VMEM
    scratch = [
        v((tok, ft), BF16), v((tp, ft), F32), v((1, 128), F32), v((sp, 128), F32),
        v((tok, 128), F32), v((2, 8, 256), F32), v((2, model, 128), BF16),
        v((2, 320, model), BF16), v((ft, 128), BF16), v((64, ft), BF16),
        v((2, 128, 128), BF16), v((2, 128, 128), BF16), v((512, model), BF16),
        v((tp, sl, 256), BF16), v((tp, sl, 256), BF16), v((tp, ht, ft), BF16),
        v((2, ht, 128), F32), v((2, ht, 320), F32), v((ht, 1), F32),
        v((nz, 2, ny, sl + sl // 2, 128), BF16), v((nx, 192, 2 * ht), BF16),
        v((3, 2, ht, 128), BF16), v((512, ht), BF16), v((ht, 512), BF16),
        v((nx, tok * sp // nx, 2 * ht), F32), v((128, tok * sp // nx), BF16),
        v((nx, 8, 2 * ht), F32),
        v((nx, 128, 2 * ht), BF16), v((nx, 128, 2 * ht), BF16),
        v((nx, 8, 2 * ht), F32), v((nx, 8, 2 * ht), F32),
        v((tp, ht, ft), BF16), v((nx, 2, ht, ft), BF16),
        dma((14 + tp,)), dma((9,)), dma((9,)), dma((tp,)), dma((tp,)), dma((tp,)), dma((tp,)),
        dma((n_z,)), dma((nz,)), dma((nz, max(ny - 1, 1))), dma((nz,)), dma((nz,)), dma((nz,)),
        dma((nx,)), dma((nx,)), dma((2,)), dma((3,)), dma((nx,)), dma((nx,)), dma((nx,)), dma((nx,)),
        dma((tp,)), dma((nx, 2)),
    ]
    hbm = pl.BlockSpec(memory_space=pl.ANY)
    specs = [hbm] * 16
    specs[5] = pl.BlockSpec(memory_space=pltpu.SMEM)
    return pl.pallas_call(
        functools.partial(kernel, cfg),
        out_shape=jax.ShapeDtypeStruct((tok, ft), BF16),
        in_specs=specs,
        out_specs=pl.BlockSpec(memory_space=pltpu.VMEM),
        scratch_shapes=scratch,
        compiler_params=pltpu.CompilerParams(
            collective_id=0, has_side_effects=True, vmem_limit_bytes=67043328
        ),
    )(
        act, gain, wq, wk.T, wv.T, sink, wlq.T, wkvd, wrope.T, lgain.reshape(1, 128), kup, vup, ow, ol, jnp.asarray(ta), jnp.asarray(tb),
    )


def solution(mesh):
    return jax.shard_map(
        functools.partial(per_device, mesh.shape["sp"] // NY),
        mesh=mesh,
        in_specs=(
            P("sp", "tp"), P(), P(None, "tp"), P(None, "tp"), P(None, "tp"), P("tp"),
            P(None, "tp"), P(), P(), P(), P(None, "tp"), P(None, "tp"), P("tp", None),
            P("tp", None),
        ),
        out_specs=P("sp", "tp"),
        check_vma=False,
    )
```

```python
import functools

import jax
import jax.numpy as jnp
import numpy as np
from jax import lax
from jax.experimental import pallas as pl
from jax.experimental.pallas import tpu as pltpu
from jax.sharding import PartitionSpec as P

HEADS_A = 16
DH = 64
WINDOW = 128
PLAIN = 128
D_ROPE = 64
EPSILON = 1e-06
ROPE_BASE = 10000.0
NY = 4
REACH = 4
LOG2E = 1.4426950408889634
MESH = pl.DeviceIdType.MESH
BF16 = jnp.bfloat16
F32 = jnp.float32

NT = (((1,), (1,)), ((), ()))
TN = (((0,), (0,)), ((), ()))


def mm(a, b, dims=(((1,), (0,)), ((), ()))):
    return lax.dot_general(a, b, dims, preferred_element_type=F32)


def z_plan(nz):
    if nz > 2 * REACH:
        near = [REACH, -REACH]
        for k in range(1, REACH):
            near += [k, -k]
        rest = nz // 2 - REACH
        return near, list(range(1, rest + 1))[::-1], [-k for k in range(1, rest)][::-1]
    half = nz // 2
    near = []
    for k in range(1, half + 1):
        near.append(k)
        if k != nz - k:
            near.append(-k)
    return near, [], []


def rotate(u, cos, sin):
    half = u.shape[1] // 2
    a, b = u[:, :half], u[:, half:]
    return jnp.concatenate([a * cos - b * sin, a * sin + b * cos], axis=1)


def kernel(
    cfg,
    act, gain, wq, wk, wv, sink, wlq, wkvd, wrope, lgain, kup, vup, ow, ol, ta, tb,
    out,
    actv, gv, lgv, tav, tbv, sinkv, wqv, wtv, kdv, krv, kupv, vupv, wall,
    kps, kpr, xb, accq, acct, sqv,
    kbuf, qt, kvb, catt, cat, sco, latt, keyb, mst, pos, por, pls, plr, rss, rsr,
    lsem, wssem, wrsem, kpssem, kprsem, xssem, xrsem, kzs, kzr, kys, kyr, kds, kdr,
    qss, qrs, hss, hrs, pss, prs, lss, lrs, rs_s, rs_r,
):
    nz, ny, nx, tok, ft, model = cfg
    tp = 2 * nx
    ht = tok // 2
    sl = tok // tp
    s = lax.axis_index("sp")
    t = lax.axis_index("tp")
    sp = nz * ny
    z, y = s // ny, lax.rem(s, ny)
    x, c = t // 2, lax.rem(t, 2)
    other = 1 - c
    mate = t + 1 - 2 * c

    near, fwd_up, fwd_down = z_plan(nz)
    n_seen = 2 * REACH + 1 if fwd_up else nz
    mine = pl.ds(pl.multiple_of(c * 128, 128), 128)
    mine_lat = pl.ds(pl.multiple_of((2 + c) * 128, 128), 128)
    theirs = pl.ds(pl.multiple_of(other * 128, 128), 128)
    theirs_lat = pl.ds(pl.multiple_of((2 + other) * 128, 128), 128)

    def at_z(dz):
        return lax.rem(z + dz + nz, nz)

    def at_y(dy):
        return lax.rem(y + dy + ny, ny)

    def rc(src, dst, ss, rs, sp_id, tp_id):
        return pltpu.make_async_remote_copy(
            src_ref=src, dst_ref=dst, send_sem=ss, recv_sem=rs,
            device_id=(sp_id, tp_id), device_id_type=MESH,
        )

    def done(ref, sem):
        pltpu.make_async_copy(ref, ref, sem).wait()

    barrier = pltpu.get_barrier_semaphore()
    n_sig = 0

    def greet(sp_id, tp_id):
        pl.semaphore_signal(barrier, inc=1, device_id=(sp_id, tp_id), device_id_type=MESH)

    for d in range(1, tp):
        greet(s, lax.rem(t + d, tp))
        n_sig += 1
    for dz in near:
        greet(at_z(dz) * ny + y, t)
        n_sig += 1
    for dy in range(1, ny):
        greet(z * ny + at_y(dy), t)
        n_sig += 1
    side = lax.rem(s + 2 * c - 1 + sp, sp)
    greet(side, mate)
    n_sig += 1
    rows = pl.ds(pl.multiple_of(t * ft, ft), ft)
    loads = [
        (act, actv), (wkvd.at[rows], kdv), (wrope.at[:, rows], krv),
    ] + [(gain.at[pl.ds(k * ft, ft)], gv.at[k]) for k in range(tp)] + [
        (lgain, lgv), (ta, tav), (tb, tbv),
        (wq, wqv.at[c]), (wk, wtv.at[c, 0:64]), (wv, wtv.at[c, 64:128]),
        (wlq, wtv.at[c, 128:320]),
        (kup, kupv.at[c]), (vup, vupv.at[c]), (ow, wall.at[mine]), (ol, wall.at[mine_lat]),
    ]
    local = [pltpu.make_async_copy(a, b, lsem.at[i]) for i, (a, b) in enumerate(loads)]
    early = 3 + tp
    for copy in local[:early]:
        copy.start()

    own_sink = jnp.concatenate(
        [jnp.full((8, 128), sink[0], F32), jnp.full((8, 128), sink[1], F32)], axis=1
    )
    sinkv[c] = own_sink

    for copy in local[:early]:
        copy.wait()
    xn = actv[...].astype(F32)
    sq0 = jnp.sum(xn * xn, axis=1, keepdims=True)
    xn = (xn * gv[pl.ds(t, 1), :]).astype(BF16)
    kps[...] = jnp.concatenate(
        [mm(xn, kdv[...]), mm(xn, krv[...], NT), jnp.broadcast_to(sq0, (tok, D_ROPE))],
        axis=1,
    ).astype(BF16).reshape(tp, sl, 256)
    kpr[pl.ds(t, 1)] = kps[pl.ds(t, 1)]
    pl.semaphore_wait(barrier, n_sig)

    def order(d):
        hop = d // 2 + 1
        if nx == 4:
            hop = jnp.where(hop == 3, 3, 3 - hop)
        return jnp.where(d < tp - 2, lax.rem((x + hop) * 2 + lax.rem(c + d, 2), tp), mate)

    def order_x(d):
        hop = d // 2 + 1
        if nx == 4:
            hop = jnp.where(hop == 1, 1, 5 - hop)
        return jnp.where(d < tp - 2, lax.rem((x + hop) * 2 + lax.rem(c + d, 2), tp), mate)

    def send_kp(d, _):
        j = order(d)
        rc(kps.at[j], kpr.at[t], kpssem.at[d], kprsem.at[t], s, j).start()
        return 0

    lax.fori_loop(0, tp - 1, send_kp, 0)

    def send_x(d, _):
        j = order_x(d)
        half = pl.ds(pl.multiple_of(lax.rem(j, 2) * ht, ht), ht)
        rc(actv.at[half], xb.at[t], xssem.at[d], xrsem.at[t], s, j).start()
        return 0

    lax.fori_loop(0, tp - 1, send_x, 0)
    for copy in local[early:]:
        copy.start()
    wsends = [
        (wq, wqv.at[c]), (wk, wtv.at[c, 0:64]), (wv, wtv.at[c, 64:128]),
        (wlq, wtv.at[c, 128:320]), (kup, kupv.at[c]), (vup, vupv.at[c]),
        (ow, wall.at[mine]), (ol, wall.at[mine_lat]), (sinkv.at[c], sinkv.at[c]),
    ]
    wdone = [
        wqv.at[other], wtv.at[other, 0:64], wtv.at[other, 64:128], wtv.at[other, 128:320],
        kupv.at[other], vupv.at[other], wall.at[theirs], wall.at[theirs_lat], sinkv.at[other],
    ]
    wcopies = [
        rc(a, b, wssem.at[i], wrsem.at[i], s, mate) for i, (a, b) in enumerate(wsends)
    ]
    for copy in wcopies:
        copy.start()

    for copy in local[early : early + 3]:
        copy.wait()
    cos_a, sin_a = tav[pl.ds(s, 1), 0:32], tav[pl.ds(s, 1), 32:64]

    def angles(start, count):
        at = pl.ds(pl.multiple_of(start, count), count)
        cos_b, sin_b = tbv[at, 0:32], tbv[at, 32:64]
        return cos_a * cos_b - sin_a * sin_b, sin_a * cos_b + cos_a * sin_b

    def wait_kp(d, _):
        j = order(d)
        done(kpr.at[j], kprsem.at[j])
        return 0

    lax.fori_loop(0, tp - 1, wait_kp, 0)
    tot = kpr[0].astype(F32)
    for j in range(1, tp):
        tot = tot + kpr[j].astype(F32)
    comp, rope, sqs = tot[:, :128], tot[:, 128:192], tot[:, 192:193]
    lat = comp * lax.rsqrt(jnp.mean(comp * comp, axis=1, keepdims=True) + EPSILON) * lgv[...]
    kcos, ksin = angles(t * sl, sl)
    kro = rotate(rope * lax.rsqrt(sqs / model + EPSILON), kcos, ksin)
    chunk = jnp.concatenate(
        [lat, jnp.concatenate([kro[: sl // 2], kro[sl // 2 :]], axis=1)], axis=0
    ).astype(BF16)
    kbuf[z, c, y] = chunk

    def z_send(dz, zs, sem):
        rc(kbuf.at[zs, c, y], kbuf.at[zs, c, y], kzs.at[sem], kzr.at[zs],
           at_z(dz) * ny + y, t).start()

    for i, dz in enumerate(near):
        z_send(dz, z, i)

    def y_send(zs):
        for dy in range(1, ny):
            rc(kbuf.at[zs, c, y], kbuf.at[zs, c, y], kys.at[zs, dy - 1], kyr.at[zs],
               z * ny + at_y(dy), t).start()

    def zs_of(j):
        far = (j + 1) // 2
        return lax.rem(z + jnp.where(lax.rem(j, 2) == 0, far, nz - far), nz)

    def step_a(j, _):
        zs = zs_of(j)
        done(kbuf.at[zs, c, y], kzr.at[zs])
        y_send(zs)
        return 0

    def step_b(j, _):
        zs = zs_of(j)
        if ny > 1:
            done(kbuf.at[zs, c, pl.ds(0, ny - 1)], kyr.at[zs])
        rc(kbuf.at[zs, c], kbuf.at[zs, c], kds.at[zs], kdr.at[zs], s, mate).start()
        return 0

    y_send(z)

    for copy in local[early + 3 : early + 7]:
        copy.wait()
    for i in range(4):
        done(wdone[i], wrsem.at[i])

    def project(xk, k, first):
        xf = xk.astype(F32)
        sq = jnp.sum(xf * xf, axis=1, keepdims=True)
        xk = (xf * gv[pl.ds(k, 1), :]).astype(BF16)
        kr = pl.ds(pl.multiple_of(k * ft, ft), ft)
        for c2 in range(2):
            term = mm(xk, wqv[c2, kr, :])
            accq[c2] = term if first else accq[c2] + term
            term = mm(xk, wtv[c2, :, kr], NT)
            acct[c2] = term if first else acct[c2] + term
        sqv[...] = sq if first else sqv[...] + sq

    own_half = pl.ds(pl.multiple_of(c * ht, ht), ht)
    project(actv[own_half, :], t, True)

    def project_next(d, _):
        k = order_x(lax.rem(d + tp - 2, tp - 1))
        done(xb.at[k], xrsem.at[k])
        project(xb[k], k, False)
        return 0

    lax.fori_loop(0, tp - 3, project_next, 0)

    if fwd_up:
        lax.fori_loop(1, n_seen - 2, step_a, 0)
        zs = at_z(-REACH)
        done(kbuf.at[zs, c, y], kzr.at[zs])
        for i, dz in enumerate(fwd_up):
            z_send(dz, zs, len(near) + i)
        y_send(zs)
        zs = at_z(REACH)
        done(kbuf.at[zs, c, y], kzr.at[zs])
        for i, dz in enumerate(fwd_down):
            z_send(dz, zs, len(near) + len(fwd_up) + i)
        y_send(zs)
    else:
        lax.fori_loop(1, nz, step_a, 0)
    lax.fori_loop(max(tp - 3, 0), tp - 1, project_next, 0)

    scale = lax.rsqrt(sqv[...] / model + EPSILON)
    local[early + 7].wait()
    done(wdone[4], wrsem.at[4])
    qcos, qsin = angles(c * ht, ht)
    factor = (PLAIN + D_ROPE) ** (-0.5) * LOG2E
    for c2 in range(2):
        ql = acct[c2, :, 128:320] * scale
        plain = ql[:, :PLAIN].astype(BF16)
        qt[x, 0:128, c2 * ht : (c2 + 1) * ht] = (mm(kupv[c2], plain, NT) * factor).astype(BF16)
        turned = rotate(ql[:, PLAIN:], qcos, qsin) * factor
        qt[x, 128:192, c2 * ht : (c2 + 1) * ht] = jnp.transpose(turned).astype(BF16)
    sides = [1, 3] if nx == 4 else list(range(1, nx))
    across = [2] if nx == 4 else []
    for i, dx in enumerate(sides + across):
        xo = lax.rem(x + dx, nx)
        rc(qt.at[x], qt.at[x], qss.at[i], qrs.at[x], s, xo * 2 + c).start()

    for c2 in range(2):
        kvb[1, c2] = (acct[c2, :, 0:128] * scale).astype(BF16)
    to_mate = rc(kvb.at[1], kvb.at[2 * c], hss.at[0], hrs.at[2 * c], s, mate)
    to_mate.start()
    to_side = rc(kvb.at[1], kvb.at[2 * other], hss.at[1], hrs.at[2 * other], side, mate)
    to_side.start()

    mst[...] = jnp.full(mst.shape, -jnp.inf, F32)
    nkeys = 2 * ny * sl
    keys_all = nz * nkeys

    def prep(i, _):
        for u in range(2):
            j = 2 * i + u
            zs = zs_of(j)
            done(kbuf.at[zs, other], kdr.at[zs])
            both = kbuf[zs].reshape(2 * ny, sl + sl // 2, 128)
            latk = both[:, :sl, :].reshape(nkeys, 128)
            rp = both[:, sl:, :]
            rk = jnp.concatenate([rp[:, :, 0:64], rp[:, :, 64:128]], axis=1)
            at = pl.ds(pl.multiple_of(j * nkeys, nkeys), nkeys)
            keyb[at, 0:128] = latk
            keyb[at, 128:192] = rk.reshape(nkeys, 64)
            latt[:, at] = jnp.transpose(latk)
        score(i, x)
        return 0

    def score(i, xp):
        at = pl.ds(pl.multiple_of(i * 2 * nkeys, 2 * nkeys), 2 * nkeys)
        sc = mm(keyb[at, :], qt[xp])
        sco[xp, at, :] = sc
        mst[xp] = jnp.maximum(mst[xp], jnp.max(sc.reshape(nkeys // 4, 8, 2 * ht), axis=0))

    def score_sides(i, _):
        for dx in sides:
            score(i, lax.rem(x + dx, nx))
        return 0

    def score_across(i, _):
        for dx in across:
            score(i, lax.rem(x + dx, nx))
        return 0

    def score_all(i, _):
        prep(i, 0)
        score_sides(i, 0)
        return score_across(i, 0)

    def wait_queries(dxs):
        for dx in dxs:
            xo = lax.rem(x + dx, nx)
            done(qt.at[xo], qrs.at[xo])

    pairs = nz // 2
    seen_p = n_seen // 2
    early_b, early_p, mid_p = min(5, n_seen), min(1, seen_p), min(2, seen_p)
    lax.fori_loop(0, early_b, step_b, 0)
    lax.fori_loop(0, early_p, prep, 0)
    lax.fori_loop(n_seen, nz, step_a, 0)
    lax.fori_loop(early_b, n_seen, step_b, 0)
    lax.fori_loop(early_p, mid_p, prep, 0)

    for i in (0, 2):
        done(kvb.at[i], hrs.at[i])
    done(wdone[8], wrsem.at[8])
    kpos = lax.broadcasted_iota(jnp.int32, (3 * ht, ht), 0)
    qpos = lax.broadcasted_iota(jnp.int32, (3 * ht, ht), 1)
    apart = jnp.abs(qpos + ht - kpos)
    place = kpos + (s * 2 + c - 1) * ht
    inside = (apart <= WINDOW) & (place >= 0) & (place < sp * tok)
    apart = apart.astype(F32)
    for c2 in range(2):
        kw = kvb[:, c2, :, 0:64].reshape(3 * ht, DH)
        vw = kvb[:, c2, :, 64:128].reshape(3 * ht, DH)
        qw = (accq[c2] * scale).astype(BF16)
        for g in range(2):
            head = (x * 2 + c2) * 2 + g
            slope = jnp.exp2(
                jnp.full((1, ht), -8.0 / (2 * tp), F32) * (head + 1).astype(F32)
            )
            sc = mm(kw, qw[:, g * DH : (g + 1) * DH], NT) * DH ** (-0.5) - slope * apart
            sc = jnp.where(inside, sc, -jnp.inf)
            snk = sinkv[c2, 0:1, g * 128 : g * 128 + 128]
            peak = jnp.maximum(jnp.max(sc, axis=0, keepdims=True), snk)
            w = jnp.exp(sc - peak)
            den = jnp.sum(w, axis=0, keepdims=True) + jnp.exp(snk - peak)
            o = mm(vw, w.astype(BF16), TN) / den
            catt[(c2 * 2 + g) * DH : (c2 * 2 + g + 1) * DH, :] = o.astype(BF16)

    lax.fori_loop(mid_p, seen_p, prep, 0)
    wait_queries(sides)
    n_two = seen_p // 2
    rest = nz - n_seen - 2 * n_two

    def sides_b(i, _):
        for u in range(2):
            score_sides(2 * i + u, 0)
        for u in range(2 if rest >= 0 else 0):
            step_b(n_seen + 2 * i + u, 0)
        return 0

    def b_all(i, _):
        step_b(n_seen + 2 * n_two + i, 0)
        return score_all(seen_p + i, 0)

    lax.fori_loop(0, n_two, sides_b, 0)
    lax.fori_loop(2 * n_two, seen_p, score_sides, 0)
    wait_queries(across)
    lax.fori_loop(0, seen_p, score_across, 0)
    lax.fori_loop(0, max(rest, 0), b_all, 0)
    lax.fori_loop(seen_p + max(rest, 0), pairs, score_all, 0)

    part = min(512, keys_all)

    def weigh(xp):
        peak = jnp.max(mst[xp], axis=0, keepdims=True)
        l8 = jnp.zeros((8, 2 * ht), F32)
        o = jnp.zeros((128, 2 * ht), F32)
        for k in range(keys_all // part):
            p = jnp.exp2(sco[xp, k * part : (k + 1) * part, :] - peak)
            l8 = l8 + jnp.sum(p.reshape(part // 8, 8, 2 * ht), axis=0)
            o = o + mm(latt[:, k * part : (k + 1) * part], p.astype(BF16))
        l = jnp.sum(l8, axis=0, keepdims=True)
        pos[xp] = (o / l).astype(BF16)
        pls[xp] = jnp.broadcast_to(peak + jnp.log(l) * LOG2E, (8, 2 * ht))

    def weigh_next(i, _):
        dx = i + 1
        if nx == 4:
            dx = jnp.where(dx == 3, 3, 3 - dx)
        xo = lax.rem(x + dx, nx)
        weigh(xo)
        rc(pls.at[xo], plr.at[x], lss.at[i], lrs.at[x], s, xo * 2 + c).start()
        rc(pos.at[xo], por.at[x], pss.at[i], prs.at[x], s, xo * 2 + c).start()
        return 0

    lax.fori_loop(0, nx - 1, weigh_next, 0)
    weigh(x)
    por[pl.ds(x, 1)] = pos[pl.ds(x, 1)]
    plr[pl.ds(x, 1)] = pls[pl.ds(x, 1)]
    for copy in local[early + 8 :]:
        copy.wait()
    for i in range(5, 8):
        done(wdone[i], wrsem.at[i])
    for dx in range(1, nx):
        xo = lax.rem(x + dx, nx)
        done(plr.at[xo], lrs.at[xo])
        done(por.at[xo], prs.at[xo])
    lse = [plr[xp, 0:1, :] for xp in range(nx)]
    top = functools.reduce(jnp.maximum, lse)
    wts = [jnp.exp2(v - top) for v in lse]
    total = functools.reduce(lambda a, b: a + b, wts)
    mixed = por[0].astype(F32) * wts[0]
    for xp in range(1, nx):
        mixed = mixed + por[xp].astype(F32) * wts[xp]
    mixed = (mixed / total).astype(BF16)
    for h in range(2):
        catt[256 + h * 128 : 256 + (h + 1) * 128, :] = mm(
            vupv[h], mixed[:, h * ht : (h + 1) * ht], TN
        ).astype(BF16)
    cat[...] = jnp.transpose(catt[...])

    def out_block(j):
        cols = pl.ds(pl.multiple_of(j * ft, ft), ft)
        return mm(cat[...], wall[:, cols]).astype(BF16)

    def send_block(d, _):
        j = order(d)
        rss[j] = out_block(j)
        rc(rss.at[j], rsr.at[x, c], rs_s.at[d], rs_r.at[x, c], s, j).start()
        return 0

    lax.fori_loop(0, tp - 1, send_block, 0)
    rsr[x, c] = out_block(t)

    def wait_block(d, _):
        j = order(tp - 2 - d)
        jx, jc = j // 2, lax.rem(j, 2)
        done(rsr.at[jx, jc], rs_r.at[jx, jc])
        return 0

    lax.fori_loop(0, tp - 1, wait_block, 0)
    for c2 in range(2):
        total = rsr[0, c2].astype(F32)
        for xp in range(1, nx):
            total = total + rsr[xp, c2].astype(F32)
        out[c2 * ht : (c2 + 1) * ht, :] = total.astype(BF16)

    def sent(d, _):
        done(kps.at[0], kpssem.at[d])
        done(xb.at[0], xssem.at[d])
        done(rss.at[0], rs_s.at[d])
        return 0

    lax.fori_loop(0, tp - 1, sent, 0)
    for copy in wcopies:
        copy.wait_send()
    for i in range(len(near) + len(fwd_up) + len(fwd_down)):
        done(kbuf.at[0, 0, 0], kzs.at[i])

    def sent_keys(zs, _):
        for dy in range(ny - 1):
            done(kbuf.at[0, 0, 0], kys.at[zs, dy])
        done(kbuf.at[0, 0], kds.at[zs])
        return 0

    lax.fori_loop(0, nz, sent_keys, 0)
    for i in range(nx - 1):
        done(qt.at[0], qss.at[i])
        done(pls.at[0], lss.at[i])
        done(pos.at[0], pss.at[i])
    to_mate.wait_send()
    to_side.wait_send()


def tables(sp, tok):
    freq = 1.0 / ROPE_BASE ** (np.arange(0, D_ROPE, 2, dtype=np.float64) / D_ROPE)

    def table(places):
        angle = places[:, None] * freq[None, :]
        flat = np.concatenate([np.cos(angle), np.sin(angle)], axis=1)
        return np.pad(flat, ((0, 0), (0, 64))).astype(np.float32)

    return table(np.arange(sp) * float(tok)), table(np.arange(tok) * 1.0)


def per_device(nz, *args):
    (act, gain, wq, wk, wv, sink, wlq, wkvd, wrope, lgain, kup, vup, ow, ol) = args
    tp, sp = lax.axis_size("tp"), lax.axis_size("sp")
    nx = tp // 2
    ny = sp // nz
    tok, ft = act.shape
    model = tp * ft
    ht, sl = tok // 2, tok // tp
    ta, tb = tables(sp, tok)
    cfg = (nz, ny, nx, tok, ft, model)
    near, up, down = z_plan(nz)
    n_z = len(near) + len(up) + len(down)
    dma = pltpu.SemaphoreType.DMA
    v = pltpu.VMEM
    scratch = [
        v((tok, ft), BF16), v((tp, ft), F32), v((1, 128), F32), v((sp, 128), F32),
        v((tok, 128), F32), v((2, 8, 256), F32), v((2, model, 128), BF16),
        v((2, 320, model), BF16), v((ft, 128), BF16), v((64, ft), BF16),
        v((2, 128, 128), BF16), v((2, 128, 128), BF16), v((512, model), BF16),
        v((tp, sl, 256), BF16), v((tp, sl, 256), BF16), v((tp, ht, ft), BF16),
        v((2, ht, 128), F32), v((2, ht, 320), F32), v((ht, 1), F32),
        v((nz, 2, ny, sl + sl // 2, 128), BF16), v((nx, 192, 2 * ht), BF16),
        v((3, 2, ht, 128), BF16), v((512, ht), BF16), v((ht, 512), BF16),
        v((nx, tok * sp // nx, 2 * ht), F32), v((128, tok * sp // nx), BF16),
        v((tok * sp // nx, 192), BF16),
        v((nx, 8, 2 * ht), F32),
        v((nx, 128, 2 * ht), BF16), v((nx, 128, 2 * ht), BF16),
        v((nx, 8, 2 * ht), F32), v((nx, 8, 2 * ht), F32),
        v((tp, ht, ft), BF16), v((nx, 2, ht, ft), BF16),
        dma((14 + tp,)), dma((9,)), dma((9,)), dma((tp,)), dma((tp,)), dma((tp,)), dma((tp,)),
        dma((n_z,)), dma((nz,)), dma((nz, max(ny - 1, 1))), dma((nz,)), dma((nz,)), dma((nz,)),
        dma((nx,)), dma((nx,)), dma((2,)), dma((3,)), dma((nx,)), dma((nx,)), dma((nx,)), dma((nx,)),
        dma((tp,)), dma((nx, 2)),
    ]
    hbm = pl.BlockSpec(memory_space=pl.ANY)
    specs = [hbm] * 16
    specs[5] = pl.BlockSpec(memory_space=pltpu.SMEM)
    return pl.pallas_call(
        functools.partial(kernel, cfg),
        out_shape=jax.ShapeDtypeStruct((tok, ft), BF16),
        in_specs=specs,
        out_specs=pl.BlockSpec(memory_space=pltpu.VMEM),
        scratch_shapes=scratch,
        compiler_params=pltpu.CompilerParams(
            collective_id=0, has_side_effects=True, vmem_limit_bytes=67043328
        ),
    )(
        act, gain, wq, wk.T, wv.T, sink, wlq.T, wkvd, wrope.T, lgain.reshape(1, 128), kup, vup, ow, ol, jnp.asarray(ta), jnp.asarray(tb),
    )


def solution(mesh):
    return jax.shard_map(
        functools.partial(per_device, mesh.shape["sp"] // NY),
        mesh=mesh,
        in_specs=(
            P("sp", "tp"), P(), P(None, "tp"), P(None, "tp"), P(None, "tp"), P("tp"),
            P(None, "tp"), P(), P(), P(), P(None, "tp"), P(None, "tp"), P("tp", None),
            P("tp", None),
        ),
        out_specs=P("sp", "tp"),
        check_vma=False,
    )
```

```python
import functools

import jax
import jax.numpy as jnp
import numpy as np
from jax import lax
from jax.experimental import pallas as pl
from jax.experimental.pallas import tpu as pltpu
from jax.sharding import PartitionSpec as P

HEADS_A = 16
DH = 64
WINDOW = 128
PLAIN = 128
D_ROPE = 64
EPSILON = 1e-06
ROPE_BASE = 10000.0
NY = 4
REACH = 4
LOG2E = 1.4426950408889634
MESH = pl.DeviceIdType.MESH
BF16 = jnp.bfloat16
F32 = jnp.float32

NT = (((1,), (1,)), ((), ()))
TN = (((0,), (0,)), ((), ()))


def mm(a, b, dims=(((1,), (0,)), ((), ()))):
    return lax.dot_general(a, b, dims, preferred_element_type=F32)


def z_plan(nz):
    if nz > 2 * REACH:
        near = [REACH, -REACH]
        for k in range(1, REACH):
            near += [k, -k]
        rest = nz // 2 - REACH
        return near, list(range(1, rest + 1))[::-1], [-k for k in range(1, rest)][::-1]
    half = nz // 2
    near = []
    for k in range(1, half + 1):
        near.append(k)
        if k != nz - k:
            near.append(-k)
    return near, [], []


def rotate(u, cos, sin):
    half = u.shape[1] // 2
    a, b = u[:, :half], u[:, half:]
    return jnp.concatenate([a * cos - b * sin, a * sin + b * cos], axis=1)


def kernel(
    cfg,
    act, gain, wq, wk, wv, sink, wlq, wkvd, wrope, lgain, kup, vup, ow, ol, ta, tb,
    out,
    actv, gv, lgv, tav, tbv, sinkm, sinkv, wqv, wtv, kdv, krv, kupv, vupv, wall,
    kps, kpr, xb, accq, acct, sqv,
    kbuf, qt, kvb, catt, cat, sco, latt, keyb, mst, pos, por, pls, plr, rss, rsr,
    lsem, wssem, wrsem, kpssem, kprsem, xssem, xrsem, kzs, kzr, kys, kyr, kds, kdr,
    qss, qrs, hss, hrs, pss, prs, lss, lrs, rs_s, rs_r,
):
    nz, ny, nx, tok, ft, model = cfg
    tp = 2 * nx
    ht = tok // 2
    sl = tok // tp
    s = lax.axis_index("sp")
    t = lax.axis_index("tp")
    sp = nz * ny
    z, y = s // ny, lax.rem(s, ny)
    x, c = t // 2, lax.rem(t, 2)
    other = 1 - c
    mate = t + 1 - 2 * c

    near, fwd_up, fwd_down = z_plan(nz)
    n_seen = 2 * REACH + 1 if fwd_up else nz
    mine = pl.ds(pl.multiple_of(c * 128, 128), 128)
    mine_lat = pl.ds(pl.multiple_of((2 + c) * 128, 128), 128)
    theirs = pl.ds(pl.multiple_of(other * 128, 128), 128)
    theirs_lat = pl.ds(pl.multiple_of((2 + other) * 128, 128), 128)

    def at_z(dz):
        return lax.rem(z + dz + nz, nz)

    def at_y(dy):
        return lax.rem(y + dy + ny, ny)

    def rc(src, dst, ss, rs, sp_id, tp_id):
        return pltpu.make_async_remote_copy(
            src_ref=src, dst_ref=dst, send_sem=ss, recv_sem=rs,
            device_id=(sp_id, tp_id), device_id_type=MESH,
        )

    def done(ref, sem):
        pltpu.make_async_copy(ref, ref, sem).wait()

    barrier = pltpu.get_barrier_semaphore()
    n_sig = 0

    def greet(sp_id, tp_id):
        pl.semaphore_signal(barrier, inc=1, device_id=(sp_id, tp_id), device_id_type=MESH)

    for d in range(1, tp):
        greet(s, lax.rem(t + d, tp))
        n_sig += 1
    for dz in near:
        greet(at_z(dz) * ny + y, t)
        n_sig += 1
    for dy in range(1, ny):
        greet(z * ny + at_y(dy), t)
        n_sig += 1
    side = lax.rem(s + 2 * c - 1 + sp, sp)
    greet(side, mate)
    n_sig += 1
    rows = pl.ds(pl.multiple_of(t * ft, ft), ft)
    loads = [
        (act, actv), (sink, sinkm), (wkvd.at[rows], kdv), (wrope.at[:, rows], krv),
    ] + [(gain.at[pl.ds(k * ft, ft)], gv.at[k]) for k in range(tp)] + [
        (lgain, lgv), (ta, tav), (tb, tbv),
        (wq, wqv.at[c]), (wk, wtv.at[c, 0:64]), (wv, wtv.at[c, 64:128]),
        (wlq, wtv.at[c, 128:320]),
        (kup, kupv.at[c]), (vup, vupv.at[c]), (ow, wall.at[mine]), (ol, wall.at[mine_lat]),
    ]
    local = [pltpu.make_async_copy(a, b, lsem.at[i]) for i, (a, b) in enumerate(loads)]
    early = 4 + tp
    for copy in local[:early]:
        copy.start()

    for copy in local[:early]:
        copy.wait()
    own_sink = jnp.concatenate(
        [jnp.full((8, 128), sinkm[0], F32), jnp.full((8, 128), sinkm[1], F32)], axis=1
    )
    sinkv[c] = own_sink

    xn = actv[...].astype(F32)
    sq0 = jnp.sum(xn * xn, axis=1, keepdims=True)
    xn = (xn * gv[pl.ds(t, 1), :]).astype(BF16)
    kps[...] = jnp.concatenate(
        [mm(xn, kdv[...]), mm(xn, krv[...], NT), jnp.broadcast_to(sq0, (tok, D_ROPE))],
        axis=1,
    ).astype(BF16).reshape(tp, sl, 256)
    kpr[pl.ds(t, 1)] = kps[pl.ds(t, 1)]
    pl.semaphore_wait(barrier, n_sig)

    def order(d):
        hop = d // 2 + 1
        if nx == 4:
            hop = jnp.where(hop == 3, 3, 3 - hop)
        return jnp.where(d < tp - 2, lax.rem((x + hop) * 2 + lax.rem(c + d, 2), tp), mate)

    def order_x(d):
        hop = d // 2 + 1
        if nx == 4:
            hop = jnp.where(hop == 1, 1, 5 - hop)
        return jnp.where(d < tp - 2, lax.rem((x + hop) * 2 + lax.rem(c + d, 2), tp), mate)

    def send_kp(d, _):
        j = order(d)
        rc(kps.at[j], kpr.at[t], kpssem.at[d], kprsem.at[t], s, j).start()
        return 0

    lax.fori_loop(0, tp - 1, send_kp, 0)

    def send_x(d, _):
        j = order_x(d)
        half = pl.ds(pl.multiple_of(lax.rem(j, 2) * ht, ht), ht)
        rc(actv.at[half], xb.at[t], xssem.at[d], xrsem.at[t], s, j).start()
        return 0

    lax.fori_loop(0, tp - 1, send_x, 0)
    for copy in local[early:]:
        copy.start()
    wsends = [
        (wq, wqv.at[c]), (wk, wtv.at[c, 0:64]), (wv, wtv.at[c, 64:128]),
        (wlq, wtv.at[c, 128:320]), (kup, kupv.at[c]), (vup, vupv.at[c]),
        (ow, wall.at[mine]), (ol, wall.at[mine_lat]), (sinkv.at[c], sinkv.at[c]),
    ]
    wdone = [
        wqv.at[other], wtv.at[other, 0:64], wtv.at[other, 64:128], wtv.at[other, 128:320],
        kupv.at[other], vupv.at[other], wall.at[theirs], wall.at[theirs_lat], sinkv.at[other],
    ]
    wcopies = [
        rc(a, b, wssem.at[i], wrsem.at[i], s, mate) for i, (a, b) in enumerate(wsends)
    ]
    for copy in wcopies:
        copy.start()

    for copy in local[early : early + 3]:
        copy.wait()
    cos_a, sin_a = tav[pl.ds(s, 1), 0:32], tav[pl.ds(s, 1), 32:64]

    def angles(start, count):
        at = pl.ds(pl.multiple_of(start, count), count)
        cos_b, sin_b = tbv[at, 0:32], tbv[at, 32:64]
        return cos_a * cos_b - sin_a * sin_b, sin_a * cos_b + cos_a * sin_b

    def wait_kp(d, _):
        j = order(d)
        done(kpr.at[j], kprsem.at[j])
        return 0

    lax.fori_loop(0, tp - 1, wait_kp, 0)
    tot = kpr[0].astype(F32)
    for j in range(1, tp):
        tot = tot + kpr[j].astype(F32)
    comp, rope, sqs = tot[:, :128], tot[:, 128:192], tot[:, 192:193]
    lat = comp * lax.rsqrt(jnp.mean(comp * comp, axis=1, keepdims=True) + EPSILON) * lgv[...]
    kcos, ksin = angles(t * sl, sl)
    kro = rotate(rope * lax.rsqrt(sqs / model + EPSILON), kcos, ksin)
    chunk = jnp.concatenate(
        [lat, jnp.concatenate([kro[: sl // 2], kro[sl // 2 :]], axis=1)], axis=0
    ).astype(BF16)
    kbuf[z, c, y] = chunk

    def z_send(dz, zs, sem):
        rc(kbuf.at[zs, c, y], kbuf.at[zs, c, y], kzs.at[sem], kzr.at[zs],
           at_z(dz) * ny + y, t).start()

    for i, dz in enumerate(near):
        z_send(dz, z, i)

    def y_send(zs):
        for dy in range(1, ny):
            rc(kbuf.at[zs, c, y], kbuf.at[zs, c, y], kys.at[zs, dy - 1], kyr.at[zs],
               z * ny + at_y(dy), t).start()

    def zs_of(j):
        far = (j + 1) // 2
        return lax.rem(z + jnp.where(lax.rem(j, 2) == 0, far, nz - far), nz)

    def step_a(j, _):
        zs = zs_of(j)
        done(kbuf.at[zs, c, y], kzr.at[zs])
        y_send(zs)
        return 0

    def step_b(j, _):
        zs = zs_of(j)
        if ny > 1:
            done(kbuf.at[zs, c, pl.ds(0, ny - 1)], kyr.at[zs])
        rc(kbuf.at[zs, c], kbuf.at[zs, c], kds.at[zs], kdr.at[zs], s, mate).start()
        return 0

    y_send(z)

    for copy in local[early + 3 : early + 7]:
        copy.wait()
    for i in range(4):
        done(wdone[i], wrsem.at[i])

    def project(xk, k, first):
        xf = xk.astype(F32)
        sq = jnp.sum(xf * xf, axis=1, keepdims=True)
        xk = (xf * gv[pl.ds(k, 1), :]).astype(BF16)
        kr = pl.ds(pl.multiple_of(k * ft, ft), ft)
        for c2 in range(2):
            term = mm(xk, wqv[c2, kr, :])
            accq[c2] = term if first else accq[c2] + term
            term = mm(xk, wtv[c2, :, kr], NT)
            acct[c2] = term if first else acct[c2] + term
        sqv[...] = sq if first else sqv[...] + sq

    own_half = pl.ds(pl.multiple_of(c * ht, ht), ht)
    project(actv[own_half, :], t, True)

    def project_next(d, _):
        k = order_x(lax.rem(d + tp - 2, tp - 1))
        done(xb.at[k], xrsem.at[k])
        project(xb[k], k, False)
        return 0

    lax.fori_loop(0, tp - 3, project_next, 0)

    first_a = min(3, n_seen - 2) if fwd_up else nz
    first_b = min(3, n_seen)
    lax.fori_loop(1, first_a, step_a, 0)
    step_b(0, 0)
    lax.fori_loop(max(tp - 3, 0), tp - 1, project_next, 0)
    if fwd_up:
        lax.fori_loop(first_a, n_seen - 2, step_a, 0)
        zs = at_z(-REACH)
        done(kbuf.at[zs, c, y], kzr.at[zs])
        for i, dz in enumerate(fwd_up):
            z_send(dz, zs, len(near) + i)
        y_send(zs)
        zs = at_z(REACH)
        done(kbuf.at[zs, c, y], kzr.at[zs])
        for i, dz in enumerate(fwd_down):
            z_send(dz, zs, len(near) + len(fwd_up) + i)
        y_send(zs)

    scale = lax.rsqrt(sqv[...] / model + EPSILON)
    local[early + 7].wait()
    done(wdone[4], wrsem.at[4])
    qcos, qsin = angles(c * ht, ht)
    factor = (PLAIN + D_ROPE) ** (-0.5) * LOG2E
    for c2 in range(2):
        ql = acct[c2, :, 128:320] * scale
        plain = ql[:, :PLAIN].astype(BF16)
        qt[0, 0:128, c2 * ht : (c2 + 1) * ht] = (mm(kupv[c2], plain, NT) * factor).astype(BF16)
        turned = rotate(ql[:, PLAIN:], qcos, qsin) * factor
        qt[0, 128:192, c2 * ht : (c2 + 1) * ht] = jnp.transpose(turned).astype(BF16)
    sides = [1, 3] if nx == 4 else list(range(1, nx))
    across = [2] if nx == 4 else []
    for i, dx in enumerate(sides + across):
        xo = lax.rem(x + dx, nx)
        rc(qt.at[0], qt.at[nx - dx], qss.at[i], qrs.at[nx - dx], s, xo * 2 + c).start()

    for c2 in range(2):
        kvb[1, c2] = (acct[c2, :, 0:128] * scale).astype(BF16)
    to_mate = rc(kvb.at[1], kvb.at[2 * c], hss.at[0], hrs.at[2 * c], s, mate)
    to_mate.start()
    to_side = rc(kvb.at[1], kvb.at[2 * other], hss.at[1], hrs.at[2 * other], side, mate)
    to_side.start()

    mst[...] = jnp.full(mst.shape, -jnp.inf, F32)
    nkeys = 2 * ny * sl
    keys_all = nz * nkeys

    def pair(i):
        return pl.ds(pl.multiple_of(i * 2 * nkeys, 2 * nkeys), 2 * nkeys)

    def take(i):
        for u in range(2):
            j = 2 * i + u
            zs = zs_of(j)
            done(kbuf.at[zs, other], kdr.at[zs])
            both = kbuf[zs].reshape(2 * ny, sl + sl // 2, 128)
            latk = both[:, :sl, :].reshape(nkeys, 128)
            rp = both[:, sl:, :]
            rk = jnp.concatenate([rp[:, :, 0:64], rp[:, :, 64:128]], axis=1)
            at = pl.ds(pl.multiple_of(j * nkeys, nkeys), nkeys)
            keyb[at, 0:128] = latk
            keyb[at, 128:192] = rk.reshape(nkeys, 64)
            latt[:, at] = jnp.transpose(latk)

    def score(i, dx):
        sc = mm(keyb[pair(i), :], qt[dx])
        sco[dx, pair(i), :] = sc
        mst[dx] = jnp.maximum(mst[dx], jnp.max(sc.reshape(nkeys // 4, 8, 2 * ht), axis=0))

    def prep(i, _):
        take(i)
        score(i, 0)
        return 0

    def rest_of(i, _):
        for dx in across + sides:
            score(i, dx)
        return 0

    def all_of(i, _):
        take(i)
        for dx in across + sides + [0]:
            score(i, dx)
        return 0

    def wait_queries(dxs):
        for dx in dxs:
            done(qt.at[dx], qrs.at[dx])

    pairs = nz // 2
    seen_p = n_seen // 2
    early_b, early_p, mid_p = min(5, n_seen), min(1, seen_p), min(2, seen_p)
    lax.fori_loop(1, first_b, step_b, 0)
    lax.fori_loop(0, early_p, prep, 0)
    lax.fori_loop(first_b, early_b, step_b, 0)
    lax.fori_loop(n_seen, nz, step_a, 0)
    lax.fori_loop(early_b, n_seen, step_b, 0)
    lax.fori_loop(early_p, mid_p, prep, 0)

    for i in (0, 2):
        done(kvb.at[i], hrs.at[i])
    done(wdone[8], wrsem.at[8])
    kpos = lax.broadcasted_iota(jnp.int32, (3 * ht, ht), 0)
    qpos = lax.broadcasted_iota(jnp.int32, (3 * ht, ht), 1)
    apart = jnp.abs(qpos + ht - kpos)
    place = kpos + (s * 2 + c - 1) * ht
    inside = (apart <= WINDOW) & (place >= 0) & (place < sp * tok)
    apart = apart.astype(F32)
    for c2 in range(2):
        kw = kvb[:, c2, :, 0:64].reshape(3 * ht, DH)
        vw = kvb[:, c2, :, 64:128].reshape(3 * ht, DH)
        qw = (accq[c2] * scale).astype(BF16)
        for g in range(2):
            head = (x * 2 + c2) * 2 + g
            slope = jnp.exp2(
                jnp.full((1, ht), -8.0 / (2 * tp), F32) * (head + 1).astype(F32)
            )
            sc = mm(kw, qw[:, g * DH : (g + 1) * DH], NT) * DH ** (-0.5) - slope * apart
            sc = jnp.where(inside, sc, -jnp.inf)
            snk = sinkv[c2, 0:1, g * 128 : g * 128 + 128]
            peak = jnp.maximum(jnp.max(sc, axis=0, keepdims=True), snk)
            w = jnp.exp(sc - peak)
            den = jnp.sum(w, axis=0, keepdims=True) + jnp.exp(snk - peak)
            o = mm(vw, w.astype(BF16), TN) / den
            catt[(c2 * 2 + g) * DH : (c2 * 2 + g + 1) * DH, :] = o.astype(BF16)

    lax.fori_loop(mid_p, seen_p, prep, 0)
    wait_queries(sides + across)
    n_two = seen_p // 2
    rest = nz - n_seen - 2 * n_two

    def rest_b(i, _):
        for u in range(2):
            rest_of(2 * i + u, 0)
        for u in range(2 if rest >= 0 else 0):
            step_b(n_seen + 2 * i + u, 0)
        return 0

    def b_all(i, _):
        step_b(n_seen + 2 * n_two + i, 0)
        return all_of(seen_p + i, 0)

    lax.fori_loop(0, n_two, rest_b, 0)
    lax.fori_loop(2 * n_two, seen_p, rest_of, 0)
    lax.fori_loop(0, max(rest, 0), b_all, 0)
    lax.fori_loop(seen_p + max(rest, 0), pairs, all_of, 0)

    part = min(1024, keys_all)

    def weigh(dx):
        peak = jnp.max(mst[dx], axis=0, keepdims=True)
        l8 = jnp.zeros((8, 2 * ht), F32)
        o = jnp.zeros((128, 2 * ht), F32)
        for k in range(keys_all // part):
            p = jnp.exp2(sco[dx, k * part : (k + 1) * part, :] - peak)
            l8 = l8 + jnp.sum(p.reshape(part // 8, 8, 2 * ht), axis=0)
            o = o + mm(latt[:, k * part : (k + 1) * part], p.astype(BF16))
        l = jnp.sum(l8, axis=0, keepdims=True)
        return (o / l).astype(BF16), jnp.broadcast_to(peak + jnp.log(l) * LOG2E, (8, 2 * ht))

    for i, dx in enumerate(across + sides):
        pos[dx], pls[dx] = weigh(dx)
        xo, back = lax.rem(x + dx, nx), nx - dx
        rc(pls.at[dx], plr.at[back], lss.at[i], lrs.at[back], s, xo * 2 + c).start()
        rc(pos.at[dx], por.at[back], pss.at[i], prs.at[back], s, xo * 2 + c).start()
    por[0], plr[0] = weigh(0)
    for copy in local[early + 8 :]:
        copy.wait()
    for i in range(5, 8):
        done(wdone[i], wrsem.at[i])
    for dx in range(1, nx):
        done(plr.at[dx], lrs.at[dx])
        done(por.at[dx], prs.at[dx])
    lse = [plr[xp, 0:1, :] for xp in range(nx)]
    top = functools.reduce(jnp.maximum, lse)
    wts = [jnp.exp2(v - top) for v in lse]
    total = functools.reduce(lambda a, b: a + b, wts)
    mixed = por[0].astype(F32) * wts[0]
    for xp in range(1, nx):
        mixed = mixed + por[xp].astype(F32) * wts[xp]
    mixed = (mixed / total).astype(BF16)
    for h in range(2):
        catt[256 + h * 128 : 256 + (h + 1) * 128, :] = mm(
            vupv[h], mixed[:, h * ht : (h + 1) * ht], TN
        ).astype(BF16)
    cat[...] = jnp.transpose(catt[...])

    def out_block(j):
        cols = pl.ds(pl.multiple_of(j * ft, ft), ft)
        return mm(cat[...], wall[:, cols]).astype(BF16)

    def send_block(d, _):
        j = order(d)
        rss[j] = out_block(j)
        rc(rss.at[j], rsr.at[x, c], rs_s.at[d], rs_r.at[x, c], s, j).start()
        return 0

    lax.fori_loop(0, tp - 1, send_block, 0)
    rsr[x, c] = out_block(t)

    def wait_block(d, _):
        j = order(tp - 2 - d)
        jx, jc = j // 2, lax.rem(j, 2)
        done(rsr.at[jx, jc], rs_r.at[jx, jc])
        return 0

    lax.fori_loop(0, tp - 1, wait_block, 0)
    for c2 in range(2):
        total = rsr[0, c2].astype(F32)
        for xp in range(1, nx):
            total = total + rsr[xp, c2].astype(F32)
        out[c2 * ht : (c2 + 1) * ht, :] = total.astype(BF16)

    def sent(d, _):
        done(kps.at[0], kpssem.at[d])
        done(xb.at[0], xssem.at[d])
        done(rss.at[0], rs_s.at[d])
        return 0

    lax.fori_loop(0, tp - 1, sent, 0)
    for copy in wcopies:
        copy.wait_send()
    for i in range(len(near) + len(fwd_up) + len(fwd_down)):
        done(kbuf.at[0, 0, 0], kzs.at[i])

    def sent_keys(zs, _):
        for dy in range(ny - 1):
            done(kbuf.at[0, 0, 0], kys.at[zs, dy])
        done(kbuf.at[0, 0], kds.at[zs])
        return 0

    lax.fori_loop(0, nz, sent_keys, 0)
    for i in range(nx - 1):
        done(qt.at[0], qss.at[i])
        done(pls.at[0], lss.at[i])
        done(pos.at[0], pss.at[i])
    to_mate.wait_send()
    to_side.wait_send()


def tables(sp, tok):
    freq = 1.0 / ROPE_BASE ** (np.arange(0, D_ROPE, 2, dtype=np.float64) / D_ROPE)

    def table(places):
        angle = places[:, None] * freq[None, :]
        flat = np.concatenate([np.cos(angle), np.sin(angle)], axis=1)
        return np.pad(flat, ((0, 0), (0, 64))).astype(np.float32)

    return table(np.arange(sp) * float(tok)), table(np.arange(tok) * 1.0)


def per_device(nz, *args):
    (act, gain, wq, wk, wv, sink, wlq, wkvd, wrope, lgain, kup, vup, ow, ol) = args
    tp, sp = lax.axis_size("tp"), lax.axis_size("sp")
    nx = tp // 2
    ny = sp // nz
    tok, ft = act.shape
    model = tp * ft
    ht, sl = tok // 2, tok // tp
    ta, tb = tables(sp, tok)
    cfg = (nz, ny, nx, tok, ft, model)
    near, up, down = z_plan(nz)
    n_z = len(near) + len(up) + len(down)
    dma = pltpu.SemaphoreType.DMA
    v = pltpu.VMEM
    scratch = [
        v((tok, ft), BF16), v((tp, ft), F32), v((1, 128), F32), v((sp, 128), F32),
        v((tok, 128), F32), pltpu.SMEM((2,), F32), v((2, 8, 256), F32), v((2, model, 128), BF16),
        v((2, 320, model), BF16), v((ft, 128), BF16), v((64, ft), BF16),
        v((2, 128, 128), BF16), v((2, 128, 128), BF16), v((512, model), BF16),
        v((tp, sl, 256), BF16), v((tp, sl, 256), BF16), v((tp, ht, ft), BF16),
        v((2, ht, 128), F32), v((2, ht, 320), F32), v((ht, 1), F32),
        v((nz, 2, ny, sl + sl // 2, 128), BF16), v((nx, 192, 2 * ht), BF16),
        v((3, 2, ht, 128), BF16), v((512, ht), BF16), v((ht, 512), BF16),
        v((nx, tok * sp // nx, 2 * ht), F32),
        v((128, tok * sp // nx), BF16), v((tok * sp // nx, 192), BF16),
        v((nx, 8, 2 * ht), F32),
        v((nx, 128, 2 * ht), BF16), v((nx, 128, 2 * ht), BF16),
        v((nx, 8, 2 * ht), F32), v((nx, 8, 2 * ht), F32),
        v((tp, ht, ft), BF16), v((nx, 2, ht, ft), BF16),
        dma((15 + tp,)), dma((9,)), dma((9,)), dma((tp,)), dma((tp,)), dma((tp,)), dma((tp,)),
        dma((n_z,)), dma((nz,)), dma((nz, max(ny - 1, 1))), dma((nz,)), dma((nz,)), dma((nz,)),
        dma((nx,)), dma((nx,)), dma((2,)), dma((3,)), dma((nx,)), dma((nx,)), dma((nx,)), dma((nx,)),
        dma((tp,)), dma((nx, 2)),
    ]
    hbm = pl.BlockSpec(memory_space=pl.ANY)
    specs = [hbm] * 16
    return pl.pallas_call(
        functools.partial(kernel, cfg),
        out_shape=jax.ShapeDtypeStruct((tok, ft), BF16),
        in_specs=specs,
        out_specs=pl.BlockSpec(memory_space=pltpu.VMEM),
        scratch_shapes=scratch,
        compiler_params=pltpu.CompilerParams(
            collective_id=0, has_side_effects=True, vmem_limit_bytes=67043328
        ),
    )(
        act, gain, wq, wk.T, wv.T, sink, wlq.T, wkvd, wrope.T, lgain.reshape(1, 128), kup, vup, ow, ol, jnp.asarray(ta), jnp.asarray(tb),
    )


def solution(mesh):
    return jax.shard_map(
        functools.partial(per_device, mesh.shape["sp"] // NY),
        mesh=mesh,
        in_specs=(
            P("sp", "tp"), P(), P(None, "tp"), P(None, "tp"), P(None, "tp"), P("tp"),
            P(None, "tp"), P(), P(), P(), P(None, "tp"), P(None, "tp"), P("tp", None),
            P("tp", None),
        ),
        out_specs=P("sp", "tp"),
        check_vma=False,
    )
```

```python
import functools

import jax
import jax.numpy as jnp
import numpy as np
from jax import lax
from jax.experimental import pallas as pl
from jax.experimental.pallas import tpu as pltpu
from jax.sharding import PartitionSpec as P

HEADS_A = 16
DH = 64
WINDOW = 128
PLAIN = 128
D_ROPE = 64
EPSILON = 1e-06
ROPE_BASE = 10000.0
NY = 4
REACH = 4
LOG2E = 1.4426950408889634
MESH = pl.DeviceIdType.MESH
BF16 = jnp.bfloat16
F32 = jnp.float32

NT = (((1,), (1,)), ((), ()))
TN = (((0,), (0,)), ((), ()))


def mm(a, b, dims=(((1,), (0,)), ((), ()))):
    return lax.dot_general(a, b, dims, preferred_element_type=F32)


def z_plan(nz):
    if nz > 2 * REACH:
        near = [REACH, -REACH]
        for k in range(1, REACH):
            near += [k, -k]
        rest = nz // 2 - REACH
        return near, list(range(1, rest + 1)), [-k for k in range(1, rest)]
    half = nz // 2
    near = []
    for k in range(1, half + 1):
        near.append(k)
        if k != nz - k:
            near.append(-k)
    return near, [], []


def rotate(u, cos, sin):
    half = u.shape[1] // 2
    a, b = u[:, :half], u[:, half:]
    return jnp.concatenate([a * cos - b * sin, a * sin + b * cos], axis=1)


def kernel(
    cfg,
    act, gain, wq, wk, wv, sink, wlq, wkvd, wrope, lgain, kup, vup, ow, ol, ta, tb,
    out,
    actv, gv, lgv, tav, tbv, sinkm, sinkv, wqv, wtv, kdv, krv, kupv, vupv, wall,
    kps, kpr, xb, accq, accl, sqv,
    kbuf, qt, kvb, catt, cat, sco, latt, keyb, mst, pos, por, pls, plr, rss, rsr,
    lsem, wssem, wrsem, kpssem, kprsem, xssem, xrsem, kzs, kzr, kys, kyr, kds, kdr,
    qss, qrs, hss, hrs, pss, prs, lss, lrs, rs_s, rs_r,
):
    nz, ny, nx, tok, ft, model = cfg
    tp = 2 * nx
    ht = tok // 2
    sl = tok // tp
    s = lax.axis_index("sp")
    t = lax.axis_index("tp")
    sp = nz * ny
    z, y = s // ny, lax.rem(s, ny)
    x, c = t // 2, lax.rem(t, 2)
    other = 1 - c
    mate = t + 1 - 2 * c

    near, fwd_up, fwd_down = z_plan(nz)
    n_seen = 2 * REACH + 1 if fwd_up else nz
    mine = pl.ds(pl.multiple_of(c * 128, 128), 128)
    mine_lat = pl.ds(pl.multiple_of((2 + c) * 128, 128), 128)
    theirs = pl.ds(pl.multiple_of(other * 128, 128), 128)
    theirs_lat = pl.ds(pl.multiple_of((2 + other) * 128, 128), 128)

    def at_z(dz):
        return lax.rem(z + dz + nz, nz)

    def at_y(dy):
        return lax.rem(y + dy + ny, ny)

    def rc(src, dst, ss, rs, sp_id, tp_id):
        return pltpu.make_async_remote_copy(
            src_ref=src, dst_ref=dst, send_sem=ss, recv_sem=rs,
            device_id=(sp_id, tp_id), device_id_type=MESH,
        )

    def done(ref, sem):
        pltpu.make_async_copy(ref, ref, sem).wait()

    barrier = pltpu.get_barrier_semaphore()
    n_sig = 0

    def greet(sp_id, tp_id):
        pl.semaphore_signal(barrier, inc=1, device_id=(sp_id, tp_id), device_id_type=MESH)

    for d in range(1, tp):
        greet(s, lax.rem(t + d, tp))
        n_sig += 1
    for dz in near:
        greet(at_z(dz) * ny + y, t)
        n_sig += 1
    for dy in range(1, ny):
        greet(z * ny + at_y(dy), t)
        n_sig += 1
    side = lax.rem(s + 2 * c - 1 + sp, sp)
    greet(side, mate)
    n_sig += 1
    rows = pl.ds(pl.multiple_of(t * ft, ft), ft)
    loads = [
        (act, actv), (sink, sinkm), (wkvd.at[rows], kdv), (wrope.at[:, rows], krv),
    ] + [(gain.at[pl.ds(k * ft, ft)], gv.at[k]) for k in range(tp)] + [
        (lgain, lgv), (ta, tav), (tb, tbv),
        (wq, wqv.at[c]), (wk, wtv.at[c, 0:64]), (wv, wtv.at[c, 64:128]),
        (wlq, wtv.at[c, 128:320]),
        (kup, kupv.at[c]), (vup, vupv.at[c]), (ow, wall.at[mine]), (ol, wall.at[mine_lat]),
    ]
    local = [pltpu.make_async_copy(a, b, lsem.at[i]) for i, (a, b) in enumerate(loads)]
    early = 4 + tp
    for copy in local[:early]:
        copy.start()

    for copy in local[:early]:
        copy.wait()
    own_sink = jnp.concatenate(
        [jnp.full((8, 128), sinkm[0], F32), jnp.full((8, 128), sinkm[1], F32)], axis=1
    )
    sinkv[c] = own_sink

    xn = actv[...].astype(F32)
    sq0 = jnp.sum(xn * xn, axis=1, keepdims=True)
    xn = (xn * gv[pl.ds(t, 1), :]).astype(BF16)
    kps[...] = jnp.concatenate(
        [mm(xn, kdv[...]), mm(xn, krv[...], NT), jnp.broadcast_to(sq0, (tok, D_ROPE))],
        axis=1,
    ).astype(BF16).reshape(tp, sl, 256)
    kpr[pl.ds(t, 1)] = kps[pl.ds(t, 1)]
    pl.semaphore_wait(barrier, n_sig)

    def order(d):
        hop = d // 2 + 1
        if nx == 4:
            hop = jnp.where(hop == 3, 3, 3 - hop)
        return jnp.where(d < tp - 2, lax.rem((x + hop) * 2 + lax.rem(c + d, 2), tp), mate)

    def order_x(d):
        hop = d // 2 + 1
        if nx == 4:
            hop = jnp.where(hop == 1, 1, 5 - hop)
        return jnp.where(d < tp - 2, lax.rem((x + hop) * 2 + lax.rem(c + d, 2), tp), mate)

    def send_kp(d, _):
        j = order(d)
        rc(kps.at[j], kpr.at[t], kpssem.at[d], kprsem.at[t], s, j).start()
        return 0

    lax.fori_loop(0, tp - 1, send_kp, 0)

    def send_x(d, _):
        j = order_x(d)
        half = pl.ds(pl.multiple_of(lax.rem(j, 2) * ht, ht), ht)
        rc(actv.at[half], xb.at[t], xssem.at[d], xrsem.at[t], s, j).start()
        return 0

    lax.fori_loop(0, tp - 1, send_x, 0)
    for copy in local[early:]:
        copy.start()
    wsends = [
        (wq, wqv.at[c]), (wk, wtv.at[c, 0:64]), (wv, wtv.at[c, 64:128]),
        (wlq, wtv.at[c, 128:320]), (kup, kupv.at[c]), (vup, vupv.at[c]),
        (ow, wall.at[mine]), (ol, wall.at[mine_lat]), (sinkv.at[c], sinkv.at[c]),
    ]
    wdone = [
        wqv.at[other], wtv.at[other, 0:64], wtv.at[other, 64:128], wtv.at[other, 128:320],
        kupv.at[other], vupv.at[other], wall.at[theirs], wall.at[theirs_lat], sinkv.at[other],
    ]
    wcopies = [
        rc(a, b, wssem.at[i], wrsem.at[i], s, mate) for i, (a, b) in enumerate(wsends)
    ]
    for copy in wcopies:
        copy.start()

    for copy in local[early : early + 3]:
        copy.wait()
    cos_a, sin_a = tav[pl.ds(s, 1), 0:32], tav[pl.ds(s, 1), 32:64]

    def angles(start, count):
        at = pl.ds(pl.multiple_of(start, count), count)
        cos_b, sin_b = tbv[at, 0:32], tbv[at, 32:64]
        return cos_a * cos_b - sin_a * sin_b, sin_a * cos_b + cos_a * sin_b

    def wait_kp(d, _):
        j = order(d)
        done(kpr.at[j], kprsem.at[j])
        return 0

    lax.fori_loop(0, tp - 1, wait_kp, 0)
    tot = kpr[0].astype(F32)
    for j in range(1, tp):
        tot = tot + kpr[j].astype(F32)
    comp, rope, sqs = tot[:, :128], tot[:, 128:192], tot[:, 192:193]
    lat = comp * lax.rsqrt(jnp.mean(comp * comp, axis=1, keepdims=True) + EPSILON) * lgv[...]
    kcos, ksin = angles(t * sl, sl)
    kro = rotate(rope * lax.rsqrt(sqs / model + EPSILON), kcos, ksin)
    chunk = jnp.concatenate(
        [lat, jnp.concatenate([kro[: sl // 2], kro[sl // 2 :]], axis=1)], axis=0
    ).astype(BF16)
    kbuf[z, c, y] = chunk

    def z_send(dz, zs, sem):
        rc(kbuf.at[zs, c, y], kbuf.at[zs, c, y], kzs.at[sem], kzr.at[zs],
           at_z(dz) * ny + y, t).start()

    for i, dz in enumerate(near):
        z_send(dz, z, i)

    def y_send(zs):
        for dy in range(1, ny):
            rc(kbuf.at[zs, c, y], kbuf.at[zs, c, y], kys.at[zs, dy - 1], kyr.at[zs],
               z * ny + at_y(dy), t).start()

    def zs_of(j):
        far = (j + 1) // 2
        return lax.rem(z + jnp.where(lax.rem(j, 2) == 0, far, nz - far), nz)

    def step_a(j, _):
        zs = zs_of(j)
        done(kbuf.at[zs, c, y], kzr.at[zs])
        y_send(zs)
        return 0

    def step_b(j, _):
        zs = zs_of(j)
        if ny > 1:
            done(kbuf.at[zs, c, pl.ds(0, ny - 1)], kyr.at[zs])
        rc(kbuf.at[zs, c], kbuf.at[zs, c], kds.at[zs], kdr.at[zs], s, mate).start()
        return 0

    y_send(z)

    for copy in local[early + 3 : early + 7]:
        copy.wait()
    for i in range(4):
        done(wdone[i], wrsem.at[i])

    def project(xk, k, first):
        xf = xk.astype(F32)
        sq = jnp.sum(xf * xf, axis=1, keepdims=True)
        xk = (xf * gv[pl.ds(k, 1), :]).astype(BF16)
        kr = pl.ds(pl.multiple_of(k * ft, ft), ft)
        for c2 in range(2):
            term = mm(xk, wtv[c2, 128:320, kr], NT)
            accl[c2] = term if first else accl[c2] + term
        xb[k] = xk
        sqv[...] = sq if first else sqv[...] + sq

    own_half = pl.ds(pl.multiple_of(c * ht, ht), ht)
    project(actv[own_half, :], t, True)

    def project_next(d, _):
        k = order_x(lax.rem(d + tp - 2, tp - 1))
        done(xb.at[k], xrsem.at[k])
        project(xb[k], k, False)
        return 0

    lax.fori_loop(0, tp - 3, project_next, 0)

    first_a = min(3, n_seen - 2) if fwd_up else nz
    first_b = min(3, n_seen)
    lax.fori_loop(1, first_a, step_a, 0)
    step_b(0, 0)
    lax.fori_loop(max(tp - 3, 0), tp - 1, project_next, 0)
    if fwd_up:
        lax.fori_loop(first_a, n_seen - 2, step_a, 0)
        zs = at_z(-REACH)
        done(kbuf.at[zs, c, y], kzr.at[zs])
        for i, dz in enumerate(fwd_up):
            z_send(dz, zs, len(near) + i)
        y_send(zs)
        zs = at_z(REACH)
        done(kbuf.at[zs, c, y], kzr.at[zs])
        for i, dz in enumerate(fwd_down):
            z_send(dz, zs, len(near) + len(fwd_up) + i)
        y_send(zs)

    scale = lax.rsqrt(sqv[...] / model + EPSILON)
    local[early + 7].wait()
    done(wdone[4], wrsem.at[4])
    qcos, qsin = angles(c * ht, ht)
    factor = (PLAIN + D_ROPE) ** (-0.5) * LOG2E
    for c2 in range(2):
        ql = accl[c2] * scale
        plain = ql[:, :PLAIN].astype(BF16)
        qt[0, 0:128, c2 * ht : (c2 + 1) * ht] = (mm(kupv[c2], plain, NT) * factor).astype(BF16)
        turned = rotate(ql[:, PLAIN:], qcos, qsin) * factor
        qt[0, 128:192, c2 * ht : (c2 + 1) * ht] = jnp.transpose(turned).astype(BF16)
    sides = [1, 3] if nx == 4 else list(range(1, nx))
    across = [2] if nx == 4 else []
    for i, dx in enumerate(sides + across):
        xo = lax.rem(x + dx, nx)
        rc(qt.at[0], qt.at[nx - dx], qss.at[i], qrs.at[nx - dx], s, xo * 2 + c).start()

    for c2 in range(2):
        kv = mm(xb[0], wtv[c2, 0:128, 0:ft], NT)
        qw = mm(xb[0], wqv[c2, 0:ft, :])
        for k in range(1, tp):
            kr = slice(k * ft, (k + 1) * ft)
            kv = kv + mm(xb[k], wtv[c2, 0:128, kr], NT)
            qw = qw + mm(xb[k], wqv[c2, kr, :])
        kvb[1, c2] = (kv * scale).astype(BF16)
        accq[c2] = qw

    mst[...] = jnp.full(mst.shape, -jnp.inf, F32)
    nkeys = 2 * ny * sl
    keys_all = nz * nkeys

    def pair(i):
        return pl.ds(pl.multiple_of(i * 2 * nkeys, 2 * nkeys), 2 * nkeys)

    def take(i):
        for u in range(2):
            j = 2 * i + u
            zs = zs_of(j)
            done(kbuf.at[zs, other], kdr.at[zs])
            both = kbuf[zs].reshape(2 * ny, sl + sl // 2, 128)
            latk = both[:, :sl, :].reshape(nkeys, 128)
            rp = both[:, sl:, :]
            rk = jnp.concatenate([rp[:, :, 0:64], rp[:, :, 64:128]], axis=1)
            at = pl.ds(pl.multiple_of(j * nkeys, nkeys), nkeys)
            keyb[at, 0:128] = latk
            keyb[at, 128:192] = rk.reshape(nkeys, 64)
            latt[:, at] = jnp.transpose(latk)

    def score(i, dx):
        sc = mm(keyb[pair(i), :], qt[dx])
        sco[dx, pair(i), :] = sc
        mst[dx] = jnp.maximum(mst[dx], jnp.max(sc.reshape(nkeys // 4, 8, 2 * ht), axis=0))

    def prep(i, _):
        take(i)
        score(i, 0)
        return 0

    def sides_of(i, _):
        for dx in sides:
            score(i, dx)
        return 0

    def across_of(i, _):
        for dx in across:
            score(i, dx)
        return 0

    def all_of(i, _):
        take(i)
        for dx in across + sides + [0]:
            score(i, dx)
        return 0

    def wait_queries(dxs):
        for dx in dxs:
            done(qt.at[dx], qrs.at[dx])

    pairs = nz // 2
    seen_p = n_seen // 2
    cut = [min(n_seen + k, nz) for k in (0, 2, 4, 6)]
    bs = [min(k, n_seen) for k in (3, 5, 7)]
    p0, p1 = min(1, seen_p), min(2, seen_p)
    lax.fori_loop(1, bs[0], step_b, 0)
    lax.fori_loop(cut[0], cut[1], step_a, 0)
    lax.fori_loop(0, p0, prep, 0)
    lax.fori_loop(bs[0], bs[1], step_b, 0)
    lax.fori_loop(cut[1], cut[2], step_a, 0)
    lax.fori_loop(bs[1], bs[2], step_b, 0)
    lax.fori_loop(cut[2], cut[3], step_a, 0)
    lax.fori_loop(p0, p1, prep, 0)

    lax.fori_loop(cut[3], nz, step_a, 0)
    to_mate = rc(kvb.at[1], kvb.at[2 * c], hss.at[0], hrs.at[2 * c], s, mate)
    to_mate.start()
    to_side = rc(kvb.at[1], kvb.at[2 * other], hss.at[1], hrs.at[2 * other], side, mate)
    to_side.start()
    lax.fori_loop(bs[2], n_seen, step_b, 0)
    lax.fori_loop(p1, seen_p, prep, 0)
    wait_queries(sides)
    n_two = seen_p // 2
    rest = nz - n_seen - 2 * n_two

    def rest_b(i, _):
        for u in range(2):
            sides_of(2 * i + u, 0)
        for u in range(2 if rest >= 0 else 0):
            step_b(n_seen + 2 * i + u, 0)
        return 0

    def b_all(i, _):
        step_b(n_seen + 2 * n_two + i, 0)
        return all_of(seen_p + i, 0)

    lax.fori_loop(0, n_two, rest_b, 0)
    lax.fori_loop(2 * n_two, seen_p, sides_of, 0)
    wait_queries(across)
    for i in range(seen_p):
        across_of(i, 0)
    lax.fori_loop(0, max(rest, 0), b_all, 0)
    lax.fori_loop(seen_p + max(rest, 0), pairs, all_of, 0)

    part = min(1024, keys_all)

    def weigh(dx):
        peak = jnp.max(mst[dx], axis=0, keepdims=True)
        l8 = jnp.zeros((8, 2 * ht), F32)
        o = jnp.zeros((128, 2 * ht), F32)
        for k in range(keys_all // part):
            p = jnp.exp2(sco[dx, k * part : (k + 1) * part, :] - peak)
            l8 = l8 + jnp.sum(p.reshape(part // 8, 8, 2 * ht), axis=0)
            o = o + mm(latt[:, k * part : (k + 1) * part], p.astype(BF16))
        l = jnp.sum(l8, axis=0, keepdims=True)
        return (o / l).astype(BF16), jnp.broadcast_to(peak + jnp.log(l) * LOG2E, (8, 2 * ht))

    for i, dx in enumerate(across + sides):
        pos[dx], pls[dx] = weigh(dx)
        xo, back = lax.rem(x + dx, nx), nx - dx
        rc(pls.at[dx], plr.at[back], lss.at[i], lrs.at[back], s, xo * 2 + c).start()
        rc(pos.at[dx], por.at[back], pss.at[i], prs.at[back], s, xo * 2 + c).start()
    por[0], plr[0] = weigh(0)

    for i in (0, 2):
        done(kvb.at[i], hrs.at[i])
    done(wdone[8], wrsem.at[8])
    kpos = lax.broadcasted_iota(jnp.int32, (3 * ht, ht), 0)
    qpos = lax.broadcasted_iota(jnp.int32, (3 * ht, ht), 1)
    apart = jnp.abs(qpos + ht - kpos)
    place = kpos + (s * 2 + c - 1) * ht
    inside = (apart <= WINDOW) & (place >= 0) & (place < sp * tok)
    apart = apart.astype(F32)
    for c2 in range(2):
        kw = kvb[:, c2, :, 0:64].reshape(3 * ht, DH)
        vw = kvb[:, c2, :, 64:128].reshape(3 * ht, DH)
        qw = (accq[c2] * scale).astype(BF16)
        for g in range(2):
            head = (x * 2 + c2) * 2 + g
            slope = jnp.exp2(
                jnp.full((1, ht), -8.0 / (2 * tp), F32) * (head + 1).astype(F32)
            )
            sc = mm(kw, qw[:, g * DH : (g + 1) * DH], NT) * DH ** (-0.5) - slope * apart
            sc = jnp.where(inside, sc, -jnp.inf)
            snk = sinkv[c2, 0:1, g * 128 : g * 128 + 128]
            peak = jnp.maximum(jnp.max(sc, axis=0, keepdims=True), snk)
            w = jnp.exp(sc - peak)
            den = jnp.sum(w, axis=0, keepdims=True) + jnp.exp(snk - peak)
            o = mm(vw, w.astype(BF16), TN) / den
            catt[(c2 * 2 + g) * DH : (c2 * 2 + g + 1) * DH, :] = o.astype(BF16)

    for copy in local[early + 8 :]:
        copy.wait()
    for i in range(5, 8):
        done(wdone[i], wrsem.at[i])
    for dx in range(1, nx):
        done(plr.at[dx], lrs.at[dx])
        done(por.at[dx], prs.at[dx])
    lse = [plr[xp, 0:1, :] for xp in range(nx)]
    top = functools.reduce(jnp.maximum, lse)
    wts = [jnp.exp2(v - top) for v in lse]
    total = functools.reduce(lambda a, b: a + b, wts)
    mixed = por[0].astype(F32) * wts[0]
    for xp in range(1, nx):
        mixed = mixed + por[xp].astype(F32) * wts[xp]
    mixed = (mixed / total).astype(BF16)
    for h in range(2):
        catt[256 + h * 128 : 256 + (h + 1) * 128, :] = mm(
            vupv[h], mixed[:, h * ht : (h + 1) * ht], TN
        ).astype(BF16)
    cat[...] = jnp.transpose(catt[...])

    def out_block(j):
        cols = pl.ds(pl.multiple_of(j * ft, ft), ft)
        return mm(cat[...], wall[:, cols]).astype(BF16)

    def send_block(d, _):
        j = order(d)
        rss[j] = out_block(j)
        rc(rss.at[j], rsr.at[x, c], rs_s.at[d], rs_r.at[x, c], s, j).start()
        return 0

    lax.fori_loop(0, tp - 1, send_block, 0)
    rsr[x, c] = out_block(t)

    def wait_block(d, _):
        j = order(tp - 2 - d)
        jx, jc = j // 2, lax.rem(j, 2)
        done(rsr.at[jx, jc], rs_r.at[jx, jc])
        return 0

    lax.fori_loop(0, tp - 1, wait_block, 0)
    for c2 in range(2):
        total = rsr[0, c2].astype(F32)
        for xp in range(1, nx):
            total = total + rsr[xp, c2].astype(F32)
        out[c2 * ht : (c2 + 1) * ht, :] = total.astype(BF16)

    def sent(d, _):
        done(kps.at[0], kpssem.at[d])
        done(xb.at[0], xssem.at[d])
        done(rss.at[0], rs_s.at[d])
        return 0

    lax.fori_loop(0, tp - 1, sent, 0)
    for copy in wcopies:
        copy.wait_send()
    for i in range(len(near) + len(fwd_up) + len(fwd_down)):
        done(kbuf.at[0, 0, 0], kzs.at[i])

    def sent_keys(zs, _):
        for dy in range(ny - 1):
            done(kbuf.at[0, 0, 0], kys.at[zs, dy])
        done(kbuf.at[0, 0], kds.at[zs])
        return 0

    lax.fori_loop(0, nz, sent_keys, 0)
    for i in range(nx - 1):
        done(qt.at[0], qss.at[i])
        done(pls.at[0], lss.at[i])
        done(pos.at[0], pss.at[i])
    to_mate.wait_send()
    to_side.wait_send()


def tables(sp, tok):
    freq = 1.0 / ROPE_BASE ** (np.arange(0, D_ROPE, 2, dtype=np.float64) / D_ROPE)

    def table(places):
        angle = places[:, None] * freq[None, :]
        flat = np.concatenate([np.cos(angle), np.sin(angle)], axis=1)
        return np.pad(flat, ((0, 0), (0, 64))).astype(np.float32)

    return table(np.arange(sp) * float(tok)), table(np.arange(tok) * 1.0)


def per_device(nz, *args):
    (act, gain, wq, wk, wv, sink, wlq, wkvd, wrope, lgain, kup, vup, ow, ol) = args
    tp, sp = lax.axis_size("tp"), lax.axis_size("sp")
    nx = tp // 2
    ny = sp // nz
    tok, ft = act.shape
    model = tp * ft
    ht, sl = tok // 2, tok // tp
    ta, tb = tables(sp, tok)
    cfg = (nz, ny, nx, tok, ft, model)
    near, up, down = z_plan(nz)
    n_z = len(near) + len(up) + len(down)
    dma = pltpu.SemaphoreType.DMA
    v = pltpu.VMEM
    scratch = [
        v((tok, ft), BF16), v((tp, ft), F32), v((1, 128), F32), v((sp, 128), F32),
        v((tok, 128), F32), pltpu.SMEM((2,), F32), v((2, 8, 256), F32), v((2, model, 128), BF16),
        v((2, 320, model), BF16), v((ft, 128), BF16), v((64, ft), BF16),
        v((2, 128, 128), BF16), v((2, 128, 128), BF16), v((512, model), BF16),
        v((tp, sl, 256), BF16), v((tp, sl, 256), BF16), v((tp, ht, ft), BF16),
        v((2, ht, 128), F32), v((2, ht, 192), F32), v((ht, 1), F32),
        v((nz, 2, ny, sl + sl // 2, 128), BF16), v((nx, 192, 2 * ht), BF16),
        v((3, 2, ht, 128), BF16), v((512, ht), BF16), v((ht, 512), BF16),
        v((nx, tok * sp // nx, 2 * ht), F32),
        v((128, tok * sp // nx), BF16), v((tok * sp // nx, 192), BF16),
        v((nx, 8, 2 * ht), F32),
        v((nx, 128, 2 * ht), BF16), v((nx, 128, 2 * ht), BF16),
        v((nx, 8, 2 * ht), F32), v((nx, 8, 2 * ht), F32),
        v((tp, ht, ft), BF16), v((nx, 2, ht, ft), BF16),
        dma((15 + tp,)), dma((9,)), dma((9,)), dma((tp,)), dma((tp,)), dma((tp,)), dma((tp,)),
        dma((n_z,)), dma((nz,)), dma((nz, max(ny - 1, 1))), dma((nz,)), dma((nz,)), dma((nz,)),
        dma((nx,)), dma((nx,)), dma((2,)), dma((3,)), dma((nx,)), dma((nx,)), dma((nx,)), dma((nx,)),
        dma((tp,)), dma((nx, 2)),
    ]
    hbm = pl.BlockSpec(memory_space=pl.ANY)
    specs = [hbm] * 16
    return pl.pallas_call(
        functools.partial(kernel, cfg),
        out_shape=jax.ShapeDtypeStruct((tok, ft), BF16),
        in_specs=specs,
        out_specs=pl.BlockSpec(memory_space=pltpu.VMEM),
        scratch_shapes=scratch,
        compiler_params=pltpu.CompilerParams(
            collective_id=0, has_side_effects=True, vmem_limit_bytes=67043328
        ),
    )(
        act, gain, wq, wk.T, wv.T, sink, wlq.T, wkvd, wrope.T, lgain.reshape(1, 128), kup, vup, ow, ol, jnp.asarray(ta), jnp.asarray(tb),
    )


def solution(mesh):
    return jax.shard_map(
        functools.partial(per_device, mesh.shape["sp"] // NY),
        mesh=mesh,
        in_specs=(
            P("sp", "tp"), P(), P(None, "tp"), P(None, "tp"), P(None, "tp"), P("tp"),
            P(None, "tp"), P(), P(), P(), P(None, "tp"), P(None, "tp"), P("tp", None),
            P("tp", None),
        ),
        out_specs=P("sp", "tp"),
        check_vma=False,
    )
```

```python
import functools

import jax
import jax.numpy as jnp
import numpy as np
from jax import lax
from jax.experimental import pallas as pl
from jax.experimental.pallas import tpu as pltpu
from jax.sharding import PartitionSpec as P

HEADS_A = 16
DH = 64
WINDOW = 128
PLAIN = 128
D_ROPE = 64
EPSILON = 1e-06
ROPE_BASE = 10000.0
NY = 4
REACH = 4
LOG2E = 1.4426950408889634
MESH = pl.DeviceIdType.MESH
BF16 = jnp.bfloat16
F32 = jnp.float32

NT = (((1,), (1,)), ((), ()))
TN = (((0,), (0,)), ((), ()))


def mm(a, b, dims=(((1,), (0,)), ((), ()))):
    return lax.dot_general(a, b, dims, preferred_element_type=F32)


def z_plan(nz):
    if nz > 2 * REACH:
        near = [REACH, -REACH]
        for k in range(1, REACH):
            near += [k, -k]
        rest = nz // 2 - REACH
        return near, list(range(1, rest + 1)), [-k for k in range(1, rest)]
    half = nz // 2
    near = []
    for k in range(1, half + 1):
        near.append(k)
        if k != nz - k:
            near.append(-k)
    return near, [], []


def rotate(u, cos, sin):
    half = u.shape[1] // 2
    a, b = u[:, :half], u[:, half:]
    return jnp.concatenate([a * cos - b * sin, a * sin + b * cos], axis=1)


def kernel(
    cfg,
    act, gain, wq, wk, wv, sink, wlq, wkvd, wrope, lgain, kup, vup, ow, ol, ta, tb,
    out,
    actv, gv, lgv, tav, tbv, sinkm, sinkv, wqv, wtv, kdv, krv, kupv, vupv, wall,
    kps, kpr, xb, accq, accl, sqv,
    kbuf, qt, kvb, catt, cat, sco, latt, keyb, mst, pos, por, pls, plr, rss, rsr,
    lsem, wssem, wrsem, kpssem, kprsem, xssem, xrsem, kzs, kzr, kys, kyr, kds, kdr,
    qss, qrs, hss, hrs, pss, prs, lss, lrs, rs_s, rs_r,
):
    nz, ny, nx, tok, ft, model = cfg
    tp = 2 * nx
    ht = tok // 2
    sl = tok // tp
    s = lax.axis_index("sp")
    t = lax.axis_index("tp")
    sp = nz * ny
    z, y = s // ny, lax.rem(s, ny)
    x, c = t // 2, lax.rem(t, 2)
    other = 1 - c
    mate = t + 1 - 2 * c

    near, fwd_up, fwd_down = z_plan(nz)
    n_seen = 2 * REACH + 1 if fwd_up else nz
    mine = pl.ds(pl.multiple_of(c * 128, 128), 128)
    mine_lat = pl.ds(pl.multiple_of((2 + c) * 128, 128), 128)
    theirs = pl.ds(pl.multiple_of(other * 128, 128), 128)
    theirs_lat = pl.ds(pl.multiple_of((2 + other) * 128, 128), 128)

    def at_z(dz):
        return lax.rem(z + dz + nz, nz)

    def at_y(dy):
        return lax.rem(y + dy + ny, ny)

    def rc(src, dst, ss, rs, sp_id, tp_id):
        return pltpu.make_async_remote_copy(
            src_ref=src, dst_ref=dst, send_sem=ss, recv_sem=rs,
            device_id=(sp_id, tp_id), device_id_type=MESH,
        )

    def done(ref, sem):
        pltpu.make_async_copy(ref, ref, sem).wait()

    barrier = pltpu.get_barrier_semaphore()
    n_sig = 0

    def greet(sp_id, tp_id):
        pl.semaphore_signal(barrier, inc=1, device_id=(sp_id, tp_id), device_id_type=MESH)

    for d in range(1, tp):
        greet(s, lax.rem(t + d, tp))
        n_sig += 1
    for dz in near:
        greet(at_z(dz) * ny + y, t)
        n_sig += 1
    for dy in range(1, ny):
        greet(z * ny + at_y(dy), t)
        n_sig += 1
    side = lax.rem(s + 2 * c - 1 + sp, sp)
    greet(side, mate)
    n_sig += 1
    rows = pl.ds(pl.multiple_of(t * ft, ft), ft)
    loads = [
        (act, actv), (sink, sinkm), (wkvd.at[rows], kdv), (wrope.at[:, rows], krv),
    ] + [(gain.at[pl.ds(k * ft, ft)], gv.at[k]) for k in range(tp)] + [
        (lgain, lgv), (ta, tav), (tb, tbv),
        (wq, wqv.at[c]), (wk, wtv.at[c, 0:64]), (wv, wtv.at[c, 64:128]),
        (wlq, wtv.at[c, 128:320]),
        (kup, kupv.at[c]), (vup, vupv.at[c]), (ow, wall.at[mine]), (ol, wall.at[mine_lat]),
    ]
    local = [pltpu.make_async_copy(a, b, lsem.at[i]) for i, (a, b) in enumerate(loads)]
    early = 4 + tp
    for copy in local[:early]:
        copy.start()

    for copy in local[:early]:
        copy.wait()
    own_sink = jnp.concatenate(
        [jnp.full((8, 128), sinkm[0], F32), jnp.full((8, 128), sinkm[1], F32)], axis=1
    )
    sinkv[c] = own_sink

    xn = actv[...].astype(F32)
    sq0 = jnp.sum(xn * xn, axis=1, keepdims=True)
    xn = (xn * gv[pl.ds(t, 1), :]).astype(BF16)
    kps[...] = jnp.concatenate(
        [mm(xn, kdv[...]), mm(xn, krv[...], NT), jnp.broadcast_to(sq0, (tok, D_ROPE))],
        axis=1,
    ).astype(BF16).reshape(tp, sl, 256)
    kpr[pl.ds(t, 1)] = kps[pl.ds(t, 1)]
    pl.semaphore_wait(barrier, n_sig)

    def order(d):
        hop = d // 2 + 1
        if nx == 4:
            hop = jnp.where(hop == 3, 3, 3 - hop)
        return jnp.where(d < tp - 2, lax.rem((x + hop) * 2 + lax.rem(c + d, 2), tp), mate)

    def order_x(d):
        hop = d // 2 + 1
        if nx == 4:
            hop = jnp.where(hop == 1, 1, 5 - hop)
        return jnp.where(d < tp - 2, lax.rem((x + hop) * 2 + lax.rem(c + d, 2), tp), mate)

    def send_kp(d, _):
        j = order(d)
        rc(kps.at[j], kpr.at[t], kpssem.at[d], kprsem.at[t], s, j).start()
        return 0

    lax.fori_loop(0, tp - 1, send_kp, 0)

    def send_x(d, _):
        j = order_x(d)
        half = pl.ds(pl.multiple_of(lax.rem(j, 2) * ht, ht), ht)
        rc(actv.at[half], xb.at[t], xssem.at[d], xrsem.at[t], s, j).start()
        return 0

    lax.fori_loop(0, tp - 1, send_x, 0)
    for copy in local[early:]:
        copy.start()
    wsends = [
        (wq, wqv.at[c]), (wk, wtv.at[c, 0:64]), (wv, wtv.at[c, 64:128]),
        (wlq, wtv.at[c, 128:320]), (kup, kupv.at[c]), (vup, vupv.at[c]),
        (ow, wall.at[mine]), (ol, wall.at[mine_lat]), (sinkv.at[c], sinkv.at[c]),
    ]
    wdone = [
        wqv.at[other], wtv.at[other, 0:64], wtv.at[other, 64:128], wtv.at[other, 128:320],
        kupv.at[other], vupv.at[other], wall.at[theirs], wall.at[theirs_lat], sinkv.at[other],
    ]
    wcopies = [
        rc(a, b, wssem.at[i], wrsem.at[i], s, mate) for i, (a, b) in enumerate(wsends)
    ]
    for copy in wcopies:
        copy.start()

    for copy in local[early : early + 3]:
        copy.wait()
    cos_a, sin_a = tav[pl.ds(s, 1), 0:32], tav[pl.ds(s, 1), 32:64]

    def angles(start, count):
        at = pl.ds(pl.multiple_of(start, count), count)
        cos_b, sin_b = tbv[at, 0:32], tbv[at, 32:64]
        return cos_a * cos_b - sin_a * sin_b, sin_a * cos_b + cos_a * sin_b

    def wait_kp(d, _):
        j = order(d)
        done(kpr.at[j], kprsem.at[j])
        return 0

    lax.fori_loop(0, tp - 1, wait_kp, 0)
    tot = kpr[0].astype(F32)
    for j in range(1, tp):
        tot = tot + kpr[j].astype(F32)
    comp, rope, sqs = tot[:, :128], tot[:, 128:192], tot[:, 192:193]
    lat = comp * lax.rsqrt(jnp.mean(comp * comp, axis=1, keepdims=True) + EPSILON) * lgv[...]
    kcos, ksin = angles(t * sl, sl)
    kro = rotate(rope * lax.rsqrt(sqs / model + EPSILON), kcos, ksin)
    chunk = jnp.concatenate(
        [lat, jnp.concatenate([kro[: sl // 2], kro[sl // 2 :]], axis=1)], axis=0
    ).astype(BF16)
    kbuf[z, c, y] = chunk

    def z_send(dz, zs, sem):
        rc(kbuf.at[zs, c, y], kbuf.at[zs, c, y], kzs.at[sem], kzr.at[zs],
           at_z(dz) * ny + y, t).start()

    for i, dz in enumerate(near):
        z_send(dz, z, i)

    def y_send(zs):
        for dy in range(1, ny):
            rc(kbuf.at[zs, c, y], kbuf.at[zs, c, y], kys.at[zs, dy - 1], kyr.at[zs],
               z * ny + at_y(dy), t).start()

    def zs_of(j):
        far = (j + 1) // 2
        return lax.rem(z + jnp.where(lax.rem(j, 2) == 0, far, nz - far), nz)

    def step_a(j, _):
        zs = zs_of(j)
        done(kbuf.at[zs, c, y], kzr.at[zs])
        y_send(zs)
        return 0

    def step_b(j, _):
        zs = zs_of(j)
        if ny > 1:
            done(kbuf.at[zs, c, pl.ds(0, ny - 1)], kyr.at[zs])
        rc(kbuf.at[zs, c], kbuf.at[zs, c], kds.at[zs], kdr.at[zs], s, mate).start()
        return 0

    y_send(z)

    for copy in local[early + 3 : early + 7]:
        copy.wait()
    for i in range(4):
        done(wdone[i], wrsem.at[i])

    def project(xk, k, first):
        xf = xk.astype(F32)
        sq = jnp.sum(xf * xf, axis=1, keepdims=True)
        xk = (xf * gv[pl.ds(k, 1), :]).astype(BF16)
        kr = pl.ds(pl.multiple_of(k * ft, ft), ft)
        for c2 in range(2):
            term = mm(xk, wtv[c2, 128:320, kr], NT)
            accl[c2] = term if first else accl[c2] + term
        xb[k] = xk
        sqv[...] = sq if first else sqv[...] + sq

    own_half = pl.ds(pl.multiple_of(c * ht, ht), ht)
    project(actv[own_half, :], t, True)

    def project_next(d, _):
        k = order_x(lax.rem(d + tp - 2, tp - 1))
        done(xb.at[k], xrsem.at[k])
        project(xb[k], k, False)
        return 0

    lax.fori_loop(0, tp - 3, project_next, 0)

    first_a = min(3, n_seen - 2) if fwd_up else nz
    first_b = min(3, n_seen)
    lax.fori_loop(1, first_a, step_a, 0)
    step_b(0, 0)
    lax.fori_loop(max(tp - 3, 0), tp - 1, project_next, 0)
    if fwd_up:
        lax.fori_loop(first_a, n_seen - 2, step_a, 0)
        zs = at_z(-REACH)
        done(kbuf.at[zs, c, y], kzr.at[zs])
        for i, dz in enumerate(fwd_up):
            z_send(dz, zs, len(near) + i)
        y_send(zs)
        zs = at_z(REACH)
        done(kbuf.at[zs, c, y], kzr.at[zs])
        for i, dz in enumerate(fwd_down):
            z_send(dz, zs, len(near) + len(fwd_up) + i)
        y_send(zs)

    scale = lax.rsqrt(sqv[...] / model + EPSILON)
    local[early + 7].wait()
    done(wdone[4], wrsem.at[4])
    qcos, qsin = angles(c * ht, ht)
    factor = (PLAIN + D_ROPE) ** (-0.5) * LOG2E
    for c2 in range(2):
        ql = accl[c2] * scale
        plain = ql[:, :PLAIN].astype(BF16)
        qt[0, 0:128, c2 * ht : (c2 + 1) * ht] = (mm(kupv[c2], plain, NT) * factor).astype(BF16)
        turned = rotate(ql[:, PLAIN:], qcos, qsin) * factor
        qt[0, 128:192, c2 * ht : (c2 + 1) * ht] = jnp.transpose(turned).astype(BF16)
    sides = [1, 3] if nx == 4 else list(range(1, nx))
    across = [2] if nx == 4 else []
    for i, dx in enumerate(sides + across):
        xo = lax.rem(x + dx, nx)
        rc(qt.at[0], qt.at[nx - dx], qss.at[i], qrs.at[nx - dx], s, xo * 2 + c).start()

    for c2 in range(2):
        kv = mm(xb[0], wtv[c2, 0:128, 0:ft], NT)
        qw = mm(xb[0], wqv[c2, 0:ft, :])
        for k in range(1, tp):
            kr = slice(k * ft, (k + 1) * ft)
            kv = kv + mm(xb[k], wtv[c2, 0:128, kr], NT)
            qw = qw + mm(xb[k], wqv[c2, kr, :])
        kvb[1, c2] = (kv * scale).astype(BF16)
        accq[c2] = qw

    mst[...] = jnp.full(mst.shape, -jnp.inf, F32)
    nkeys = 2 * ny * sl
    keys_all = nz * nkeys

    def pair(i):
        return pl.ds(pl.multiple_of(i * 2 * nkeys, 2 * nkeys), 2 * nkeys)

    def take(i):
        for u in range(2):
            j = 2 * i + u
            zs = zs_of(j)
            done(kbuf.at[zs, other], kdr.at[zs])
            both = kbuf[zs].reshape(2 * ny, sl + sl // 2, 128)
            latk = both[:, :sl, :].reshape(nkeys, 128)
            rp = both[:, sl:, :]
            rk = jnp.concatenate([rp[:, :, 0:64], rp[:, :, 64:128]], axis=1)
            at = pl.ds(pl.multiple_of(j * nkeys, nkeys), nkeys)
            keyb[at, 0:128] = latk
            keyb[at, 128:192] = rk.reshape(nkeys, 64)
            latt[:, at] = jnp.transpose(latk)

    def score(i, dx):
        sc = mm(keyb[pair(i), :], qt[dx])
        sco[dx, pair(i), :] = sc
        mst[dx] = jnp.maximum(mst[dx], jnp.max(sc.reshape(nkeys // 4, 8, 2 * ht), axis=0))

    def prep(i, _):
        take(i)
        score(i, 0)
        return 0

    def sides_of(i, _):
        for dx in sides:
            score(i, dx)
        return 0

    def across_of(i, _):
        for dx in across:
            score(i, dx)
        return 0

    def all_of(i, _):
        take(i)
        for dx in across + sides + [0]:
            score(i, dx)
        return 0

    def wait_queries(dxs):
        for dx in dxs:
            done(qt.at[dx], qrs.at[dx])

    pairs = nz // 2
    seen_p = n_seen // 2
    cut = [min(n_seen + k, nz) for k in (0, 2, 4, 6)]
    bs = [min(k, n_seen) for k in (3, 5, 7)]
    p0, p1 = min(1, seen_p), min(2, seen_p)
    lax.fori_loop(1, bs[0], step_b, 0)
    lax.fori_loop(cut[0], cut[1], step_a, 0)
    lax.fori_loop(0, p0, prep, 0)
    lax.fori_loop(bs[0], bs[1], step_b, 0)
    lax.fori_loop(cut[1], cut[2], step_a, 0)
    lax.fori_loop(bs[1], bs[2], step_b, 0)
    lax.fori_loop(cut[2], cut[3], step_a, 0)
    lax.fori_loop(p0, p1, prep, 0)

    lax.fori_loop(cut[3], nz, step_a, 0)
    to_mate = rc(kvb.at[1], kvb.at[2 * c], hss.at[0], hrs.at[2 * c], s, mate)
    to_mate.start()
    to_side = rc(kvb.at[1], kvb.at[2 * other], hss.at[1], hrs.at[2 * other], side, mate)
    to_side.start()
    lax.fori_loop(bs[2], n_seen, step_b, 0)
    lax.fori_loop(p1, seen_p, prep, 0)
    wait_queries(sides)
    n_two = seen_p // 2
    rest = nz - n_seen - 2 * n_two

    def rest_b(i, _):
        for u in range(2):
            sides_of(2 * i + u, 0)
        for u in range(2 if rest >= 0 else 0):
            step_b(n_seen + 2 * i + u, 0)
        return 0

    def b_all(i, _):
        step_b(n_seen + 2 * n_two + i, 0)
        return all_of(seen_p + i, 0)

    lax.fori_loop(0, n_two, rest_b, 0)
    lax.fori_loop(2 * n_two, seen_p, sides_of, 0)
    wait_queries(across)
    for i in range(seen_p):
        across_of(i, 0)
    lax.fori_loop(0, max(rest, 0), b_all, 0)
    lax.fori_loop(seen_p + max(rest, 0), pairs, all_of, 0)

    part = min(1024, keys_all)

    def weigh(dx):
        peak = jnp.max(mst[dx], axis=0, keepdims=True)
        l8 = jnp.zeros((8, 2 * ht), F32)
        o = jnp.zeros((128, 2 * ht), F32)
        for k in range(keys_all // part):
            p = jnp.exp2(sco[dx, k * part : (k + 1) * part, :] - peak)
            l8 = l8 + jnp.sum(p.reshape(part // 8, 8, 2 * ht), axis=0)
            o = o + mm(latt[:, k * part : (k + 1) * part], p.astype(BF16))
        l = jnp.sum(l8, axis=0, keepdims=True)
        return (o / l).astype(BF16), jnp.broadcast_to(peak + jnp.log(l) * LOG2E, (8, 2 * ht))

    for i, dx in enumerate(across + sides):
        pos[dx], pls[dx] = weigh(dx)
        xo, back = lax.rem(x + dx, nx), nx - dx
        rc(pls.at[dx], plr.at[back], lss.at[i], lrs.at[back], s, xo * 2 + c).start()
        rc(pos.at[dx], por.at[back], pss.at[i], prs.at[back], s, xo * 2 + c).start()
    por[0], plr[0] = weigh(0)

    for i in (0, 2):
        done(kvb.at[i], hrs.at[i])
    done(wdone[8], wrsem.at[8])
    kpos = lax.broadcasted_iota(jnp.int32, (3 * ht, ht), 0)
    qpos = lax.broadcasted_iota(jnp.int32, (3 * ht, ht), 1)
    apart = jnp.abs(qpos + ht - kpos)
    place = kpos + (s * 2 + c - 1) * ht
    inside = (apart <= WINDOW) & (place >= 0) & (place < sp * tok)
    apart = apart.astype(F32)
    for c2 in range(2):
        kw = kvb[:, c2, :, 0:64].reshape(3 * ht, DH)
        vw = kvb[:, c2, :, 64:128].reshape(3 * ht, DH)
        qw = (accq[c2] * scale).astype(BF16)
        for g in range(2):
            head = (x * 2 + c2) * 2 + g
            slope = jnp.exp2(
                jnp.full((1, ht), -8.0 / (2 * tp), F32) * (head + 1).astype(F32)
            )
            sc = mm(kw, qw[:, g * DH : (g + 1) * DH], NT) * DH ** (-0.5) - slope * apart
            sc = jnp.where(inside, sc, -jnp.inf)
            snk = sinkv[c2, 0:1, g * 128 : g * 128 + 128]
            peak = jnp.maximum(jnp.max(sc, axis=0, keepdims=True), snk)
            w = jnp.exp(sc - peak)
            den = jnp.sum(w, axis=0, keepdims=True) + jnp.exp(snk - peak)
            o = mm(vw, w.astype(BF16), TN) / den
            catt[(c2 * 2 + g) * DH : (c2 * 2 + g + 1) * DH, :] = o.astype(BF16)

    for copy in local[early + 8 :]:
        copy.wait()
    for i in range(5, 8):
        done(wdone[i], wrsem.at[i])
    for dx in range(1, nx):
        done(plr.at[dx], lrs.at[dx])
        done(por.at[dx], prs.at[dx])
    lse = [plr[xp, 0:1, :] for xp in range(nx)]
    top = functools.reduce(jnp.maximum, lse)
    wts = [jnp.exp2(v - top) for v in lse]
    total = functools.reduce(lambda a, b: a + b, wts)
    mixed = por[0].astype(F32) * wts[0]
    for xp in range(1, nx):
        mixed = mixed + por[xp].astype(F32) * wts[xp]
    mixed = (mixed / total).astype(BF16)
    for h in range(2):
        catt[256 + h * 128 : 256 + (h + 1) * 128, :] = mm(
            vupv[h], mixed[:, h * ht : (h + 1) * ht], TN
        ).astype(BF16)
    cat[...] = jnp.transpose(catt[...])

    def out_block(j):
        cols = pl.ds(pl.multiple_of(j * ft, ft), ft)
        return mm(cat[...], wall[:, cols]).astype(BF16)

    def send_block(d, _):
        j = order(d)
        rss[j] = out_block(j)
        rc(rss.at[j], rsr.at[x, c], rs_s.at[d], rs_r.at[x, c], s, j).start()
        return 0

    lax.fori_loop(0, tp - 1, send_block, 0)
    rsr[x, c] = out_block(t)

    def wait_block(d, _):
        j = order(tp - 2 - d)
        jx, jc = j // 2, lax.rem(j, 2)
        done(rsr.at[jx, jc], rs_r.at[jx, jc])
        return 0

    lax.fori_loop(0, tp - 1, wait_block, 0)
    for c2 in range(2):
        total = rsr[0, c2].astype(F32)
        for xp in range(1, nx):
            total = total + rsr[xp, c2].astype(F32)
        out[c2 * ht : (c2 + 1) * ht, :] = total.astype(BF16)

    def sent(d, _):
        done(kps.at[0], kpssem.at[d])
        done(xb.at[0], xssem.at[d])
        done(rss.at[0], rs_s.at[d])
        return 0

    lax.fori_loop(0, tp - 1, sent, 0)
    for copy in wcopies:
        copy.wait_send()
    for i in range(len(near) + len(fwd_up) + len(fwd_down)):
        done(kbuf.at[0, 0, 0], kzs.at[i])

    def sent_keys(zs, _):
        for dy in range(ny - 1):
            done(kbuf.at[0, 0, 0], kys.at[zs, dy])
        done(kbuf.at[0, 0], kds.at[zs])
        return 0

    lax.fori_loop(0, nz, sent_keys, 0)
    for i in range(nx - 1):
        done(qt.at[0], qss.at[i])
        done(pls.at[0], lss.at[i])
        done(pos.at[0], pss.at[i])
    to_mate.wait_send()
    to_side.wait_send()


def tables(sp, tok):
    freq = 1.0 / ROPE_BASE ** (np.arange(0, D_ROPE, 2, dtype=np.float64) / D_ROPE)

    def table(places):
        angle = places[:, None] * freq[None, :]
        flat = np.concatenate([np.cos(angle), np.sin(angle)], axis=1)
        return np.pad(flat, ((0, 0), (0, 64))).astype(np.float32)

    return table(np.arange(sp) * float(tok)), table(np.arange(tok) * 1.0)


def per_device(nz, *args):
    (act, gain, wq, wk, wv, sink, wlq, wkvd, wrope, lgain, kup, vup, ow, ol) = args
    tp, sp = lax.axis_size("tp"), lax.axis_size("sp")
    nx = tp // 2
    ny = sp // nz
    tok, ft = act.shape
    model = tp * ft
    ht, sl = tok // 2, tok // tp
    ta, tb = tables(sp, tok)
    cfg = (nz, ny, nx, tok, ft, model)
    near, up, down = z_plan(nz)
    n_z = len(near) + len(up) + len(down)
    dma = pltpu.SemaphoreType.DMA
    v = pltpu.VMEM
    scratch = [
        v((tok, ft), BF16), v((tp, ft), F32), v((1, 128), F32), v((sp, 128), F32),
        v((tok, 128), F32), pltpu.SMEM((2,), F32), v((2, 8, 256), F32), v((2, model, 128), BF16),
        v((2, 320, model), BF16), v((ft, 128), BF16), v((64, ft), BF16),
        v((2, 128, 128), BF16), v((2, 128, 128), BF16), v((512, model), BF16),
        v((tp, sl, 256), BF16), v((tp, sl, 256), BF16), v((tp, ht, ft), BF16),
        v((2, ht, 128), F32), v((2, ht, 192), F32), v((ht, 1), F32),
        v((nz, 2, ny, sl + sl // 2, 128), BF16), v((nx, 192, 2 * ht), BF16),
        v((3, 2, ht, 128), BF16), v((512, ht), BF16), v((ht, 512), BF16),
        v((nx, tok * sp // nx, 2 * ht), F32),
        v((128, tok * sp // nx), BF16), v((tok * sp // nx, 192), BF16),
        v((nx, 8, 2 * ht), F32),
        v((nx, 128, 2 * ht), BF16), v((nx, 128, 2 * ht), BF16),
        v((nx, 8, 2 * ht), F32), v((nx, 8, 2 * ht), F32),
        v((tp, ht, ft), BF16), v((nx, 2, ht, ft), BF16),
        dma((15 + tp,)), dma((9,)), dma((9,)), dma((tp,)), dma((tp,)), dma((tp,)), dma((tp,)),
        dma((n_z,)), dma((nz,)), dma((nz, max(ny - 1, 1))), dma((nz,)), dma((nz,)), dma((nz,)),
        dma((nx,)), dma((nx,)), dma((2,)), dma((3,)), dma((nx,)), dma((nx,)), dma((nx,)), dma((nx,)),
        dma((tp,)), dma((nx, 2)),
    ]
    keep = lambda a: pltpu.with_memory_space_constraint(a, pltpu.HBM)
    hbm = pl.BlockSpec(memory_space=pltpu.HBM)
    specs = [hbm] * 16
    return pl.pallas_call(
        functools.partial(kernel, cfg),
        out_shape=jax.ShapeDtypeStruct((tok, ft), BF16),
        in_specs=specs,
        out_specs=pl.BlockSpec(memory_space=pltpu.VMEM),
        scratch_shapes=scratch,
        compiler_params=pltpu.CompilerParams(
            collective_id=0, has_side_effects=True, vmem_limit_bytes=44000 * 1024
        ),
    )(
        *map(
            keep,
            (
                act, gain, wq, wk.T, wv.T, sink, wlq.T, wkvd, wrope.T, lgain.reshape(1, 128),
                kup, vup, ow, ol, jnp.asarray(ta), jnp.asarray(tb),
            ),
        )
    )


def solution(mesh):
    return jax.shard_map(
        functools.partial(per_device, mesh.shape["sp"] // NY),
        mesh=mesh,
        in_specs=(
            P("sp", "tp"), P(), P(None, "tp"), P(None, "tp"), P(None, "tp"), P("tp"),
            P(None, "tp"), P(), P(), P(), P(None, "tp"), P(None, "tp"), P("tp", None),
            P("tp", None),
        ),
        out_specs=P("sp", "tp"),
        check_vma=False,
    )
```

```python
import functools

import jax
import jax.numpy as jnp
import numpy as np
from jax import lax
from jax.experimental import pallas as pl
from jax.experimental.pallas import tpu as pltpu
from jax.sharding import PartitionSpec as P

HEADS_A = 16
DH = 64
WINDOW = 128
PLAIN = 128
D_ROPE = 64
EPSILON = 1e-06
ROPE_BASE = 10000.0
NY = 4
REACH = 4
LOG2E = 1.4426950408889634
MESH = pl.DeviceIdType.MESH
BF16 = jnp.bfloat16
F32 = jnp.float32

NT = (((1,), (1,)), ((), ()))
TN = (((0,), (0,)), ((), ()))


def mm(a, b, dims=(((1,), (0,)), ((), ()))):
    return lax.dot_general(a, b, dims, preferred_element_type=F32)


def z_plan(nz):
    if nz > 2 * REACH:
        near = [REACH, -REACH]
        for k in range(1, REACH):
            near += [k, -k]
        rest = nz // 2 - REACH
        return near, list(range(1, rest + 1)), [-k for k in range(1, rest)]
    half = nz // 2
    near = []
    for k in range(1, half + 1):
        near.append(k)
        if k != nz - k:
            near.append(-k)
    return near, [], []


def rotate(u, cos, sin):
    half = u.shape[1] // 2
    a, b = u[:, :half], u[:, half:]
    return jnp.concatenate([a * cos - b * sin, a * sin + b * cos], axis=1)


def kernel(
    cfg,
    act, gain, wq, wk, wv, sink, wlq, wkvd, wrope, lgain, kup, vup, ow, ol, ta, tb,
    out,
    actv, gv, lgv, tav, tbv, sinkm, sinkv, wqv, wtv, kdv, krv, kupv, vupv, wall,
    kps, kpr, xb, accq, accl, sqv,
    kbuf, qt, kvb, catt, cat, sco, latt, keyb, mst, pos, por, pls, plr, rss, rsr,
    lsem, wssem, wrsem, kpssem, kprsem, xssem, xrsem, kzs, kzr, kys, kyr, kds, kdr,
    qss, qrs, hss, hrs, pss, prs, lss, lrs, rs_s, rs_r,
):
    nz, ny, nx, tok, ft, model = cfg
    tp = 2 * nx
    ht = tok // 2
    sl = tok // tp
    s = lax.axis_index("sp")
    t = lax.axis_index("tp")
    sp = nz * ny
    z, y = s // ny, lax.rem(s, ny)
    x, c = t // 2, lax.rem(t, 2)
    other = 1 - c
    mate = t + 1 - 2 * c

    near, fwd_up, fwd_down = z_plan(nz)
    n_seen = 2 * REACH + 1 if fwd_up else nz
    mine = pl.ds(pl.multiple_of(c * 128, 128), 128)
    mine_lat = pl.ds(pl.multiple_of((2 + c) * 128, 128), 128)
    theirs = pl.ds(pl.multiple_of(other * 128, 128), 128)
    theirs_lat = pl.ds(pl.multiple_of((2 + other) * 128, 128), 128)

    def at_z(dz):
        return lax.rem(z + dz + nz, nz)

    def at_y(dy):
        return lax.rem(y + dy + ny, ny)

    def rc(src, dst, ss, rs, sp_id, tp_id):
        return pltpu.make_async_remote_copy(
            src_ref=src, dst_ref=dst, send_sem=ss, recv_sem=rs,
            device_id=(sp_id, tp_id), device_id_type=MESH,
        )

    def done(ref, sem):
        pltpu.make_async_copy(ref, ref, sem).wait()

    barrier = pltpu.get_barrier_semaphore()
    n_sig = 0

    def greet(sp_id, tp_id):
        pl.semaphore_signal(barrier, inc=1, device_id=(sp_id, tp_id), device_id_type=MESH)

    for dz in near:
        greet(at_z(dz) * ny + y, t)
        n_sig += 1
    for d in range(1, tp):
        greet(s, lax.rem(t + d, tp))
        n_sig += 1
    for dy in range(1, ny):
        greet(z * ny + at_y(dy), t)
        n_sig += 1
    side = lax.rem(s + 2 * c - 1 + sp, sp)
    greet(side, mate)
    n_sig += 1
    rows = pl.ds(pl.multiple_of(t * ft, ft), ft)
    loads = [
        (act, actv), (sink, sinkm), (wkvd.at[rows], kdv), (wrope.at[:, rows], krv),
    ] + [(gain.at[pl.ds(k * ft, ft)], gv.at[k]) for k in range(tp)] + [
        (lgain, lgv), (ta, tav), (tb, tbv),
        (wq, wqv.at[c]), (wk, wtv.at[c, 0:64]), (wv, wtv.at[c, 64:128]),
        (wlq, wtv.at[c, 128:320]),
        (kup, kupv.at[c]), (vup, vupv.at[c]), (ow, wall.at[mine]), (ol, wall.at[mine_lat]),
    ]
    local = [pltpu.make_async_copy(a, b, lsem.at[i]) for i, (a, b) in enumerate(loads)]
    early = 4 + tp
    for copy in local[:early]:
        copy.start()

    for copy in local[:early]:
        copy.wait()
    own_sink = jnp.concatenate(
        [jnp.full((8, 128), sinkm[0], F32), jnp.full((8, 128), sinkm[1], F32)], axis=1
    )
    sinkv[c] = own_sink

    xn = actv[...].astype(F32)
    sq0 = jnp.sum(xn * xn, axis=1, keepdims=True)
    xn = (xn * gv[pl.ds(t, 1), :]).astype(BF16)
    kps[...] = jnp.concatenate(
        [mm(xn, kdv[...]), mm(xn, krv[...], NT), jnp.broadcast_to(sq0, (tok, D_ROPE))],
        axis=1,
    ).astype(BF16).reshape(tp, sl, 256)
    kpr[pl.ds(t, 1)] = kps[pl.ds(t, 1)]
    pl.semaphore_wait(barrier, n_sig)

    def order(d):
        hop = d // 2 + 1
        if nx == 4:
            hop = jnp.where(hop == 3, 3, 3 - hop)
        return jnp.where(d < tp - 2, lax.rem((x + hop) * 2 + lax.rem(c + d, 2), tp), mate)

    def order_x(d):
        hop = d // 2 + 1
        if nx == 4:
            hop = jnp.where(hop == 1, 1, 5 - hop)
        return jnp.where(d < tp - 2, lax.rem((x + hop) * 2 + lax.rem(c + d, 2), tp), mate)

    def send_kp(d, _):
        j = order(d)
        rc(kps.at[j], kpr.at[t], kpssem.at[d], kprsem.at[t], s, j).start()
        return 0

    lax.fori_loop(0, tp - 1, send_kp, 0)

    def send_x(d, _):
        j = order_x(d)
        half = pl.ds(pl.multiple_of(lax.rem(j, 2) * ht, ht), ht)
        rc(actv.at[half], xb.at[t], xssem.at[d], xrsem.at[t], s, j).start()
        return 0

    lax.fori_loop(0, tp - 1, send_x, 0)
    for copy in local[early:]:
        copy.start()
    wsends = [
        (wq, wqv.at[c]), (wk, wtv.at[c, 0:64]), (wv, wtv.at[c, 64:128]),
        (wlq, wtv.at[c, 128:320]), (kup, kupv.at[c]), (vup, vupv.at[c]),
        (ow, wall.at[mine]), (ol, wall.at[mine_lat]), (sinkv.at[c], sinkv.at[c]),
    ]
    wdone = [
        wqv.at[other], wtv.at[other, 0:64], wtv.at[other, 64:128], wtv.at[other, 128:320],
        kupv.at[other], vupv.at[other], wall.at[theirs], wall.at[theirs_lat], sinkv.at[other],
    ]
    wcopies = [
        rc(a, b, wssem.at[i], wrsem.at[i], s, mate) for i, (a, b) in enumerate(wsends)
    ]
    for copy in wcopies:
        copy.start()

    for copy in local[early : early + 3]:
        copy.wait()
    cos_a, sin_a = tav[pl.ds(s, 1), 0:32], tav[pl.ds(s, 1), 32:64]

    def angles(start, count):
        at = pl.ds(pl.multiple_of(start, count), count)
        cos_b, sin_b = tbv[at, 0:32], tbv[at, 32:64]
        return cos_a * cos_b - sin_a * sin_b, sin_a * cos_b + cos_a * sin_b

    def wait_kp(d, _):
        j = order(d)
        done(kpr.at[j], kprsem.at[j])
        return 0

    lax.fori_loop(0, tp - 1, wait_kp, 0)
    tot = kpr[0].astype(F32)
    for j in range(1, tp):
        tot = tot + kpr[j].astype(F32)
    comp, rope, sqs = tot[:, :128], tot[:, 128:192], tot[:, 192:193]
    lat = comp * lax.rsqrt(jnp.mean(comp * comp, axis=1, keepdims=True) + EPSILON) * lgv[...]
    kcos, ksin = angles(t * sl, sl)
    kro = rotate(rope * lax.rsqrt(sqs / model + EPSILON), kcos, ksin)
    chunk = jnp.concatenate(
        [lat, jnp.concatenate([kro[: sl // 2], kro[sl // 2 :]], axis=1)], axis=0
    ).astype(BF16)
    kbuf[z, c, y] = chunk

    def z_send(dz, zs, sem):
        rc(kbuf.at[zs, c, y], kbuf.at[zs, c, y], kzs.at[sem], kzr.at[zs],
           at_z(dz) * ny + y, t).start()

    for i, dz in enumerate(near):
        z_send(dz, z, i)

    def y_send(zs):
        for dy in range(1, ny):
            rc(kbuf.at[zs, c, y], kbuf.at[zs, c, y], kys.at[zs, dy - 1], kyr.at[zs],
               z * ny + at_y(dy), t).start()

    def zs_of(j):
        far = (j + 1) // 2
        return lax.rem(z + jnp.where(lax.rem(j, 2) == 0, far, nz - far), nz)

    def step_a(j, _):
        zs = zs_of(j)
        done(kbuf.at[zs, c, y], kzr.at[zs])
        y_send(zs)
        return 0

    def step_b(j, _):
        zs = zs_of(j)
        if ny > 1:
            done(kbuf.at[zs, c, pl.ds(0, ny - 1)], kyr.at[zs])
        rc(kbuf.at[zs, c], kbuf.at[zs, c], kds.at[zs], kdr.at[zs], s, mate).start()
        return 0

    y_send(z)

    for copy in local[early + 3 : early + 7]:
        copy.wait()
    for i in range(4):
        done(wdone[i], wrsem.at[i])

    def project(xk, k, first):
        xf = xk.astype(F32)
        sq = jnp.sum(xf * xf, axis=1, keepdims=True)
        xk = (xf * gv[pl.ds(k, 1), :]).astype(BF16)
        kr = pl.ds(pl.multiple_of(k * ft, ft), ft)
        for c2 in range(2):
            term = mm(xk, wtv[c2, 128:320, kr], NT)
            accl[c2] = term if first else accl[c2] + term
        xb[k] = xk
        sqv[...] = sq if first else sqv[...] + sq

    own_half = pl.ds(pl.multiple_of(c * ht, ht), ht)
    project(actv[own_half, :], t, True)

    def project_next(d, _):
        k = order_x(lax.rem(d + tp - 2, tp - 1))
        done(xb.at[k], xrsem.at[k])
        project(xb[k], k, False)
        return 0

    lax.fori_loop(0, tp - 3, project_next, 0)

    first_a = min(3, n_seen - 2) if fwd_up else nz
    first_b = min(3, n_seen)
    lax.fori_loop(1, first_a, step_a, 0)
    step_b(0, 0)
    lax.fori_loop(max(tp - 3, 0), tp - 1, project_next, 0)
    if fwd_up:
        lax.fori_loop(first_a, n_seen - 2, step_a, 0)
        zs = at_z(-REACH)
        done(kbuf.at[zs, c, y], kzr.at[zs])
        for i, dz in enumerate(fwd_up):
            z_send(dz, zs, len(near) + i)
        y_send(zs)
        zs = at_z(REACH)
        done(kbuf.at[zs, c, y], kzr.at[zs])
        for i, dz in enumerate(fwd_down):
            z_send(dz, zs, len(near) + len(fwd_up) + i)
        y_send(zs)

    scale = lax.rsqrt(sqv[...] / model + EPSILON)
    local[early + 7].wait()
    done(wdone[4], wrsem.at[4])
    qcos, qsin = angles(c * ht, ht)
    factor = (PLAIN + D_ROPE) ** (-0.5) * LOG2E
    for c2 in range(2):
        ql = accl[c2] * scale
        plain = ql[:, :PLAIN].astype(BF16)
        qt[0, 0:128, c2 * ht : (c2 + 1) * ht] = (mm(kupv[c2], plain, NT) * factor).astype(BF16)
        turned = rotate(ql[:, PLAIN:], qcos, qsin) * factor
        qt[0, 128:192, c2 * ht : (c2 + 1) * ht] = jnp.transpose(turned).astype(BF16)
    sides = [1, 3] if nx == 4 else list(range(1, nx))
    across = [2] if nx == 4 else []
    for i, dx in enumerate(sides + across):
        xo = lax.rem(x + dx, nx)
        rc(qt.at[0], qt.at[nx - dx], qss.at[i], qrs.at[nx - dx], s, xo * 2 + c).start()

    for c2 in range(2):
        kv = mm(xb[0], wtv[c2, 0:128, 0:ft], NT)
        qw = mm(xb[0], wqv[c2, 0:ft, :])
        for k in range(1, tp):
            kr = slice(k * ft, (k + 1) * ft)
            kv = kv + mm(xb[k], wtv[c2, 0:128, kr], NT)
            qw = qw + mm(xb[k], wqv[c2, kr, :])
        kvb[1, c2] = (kv * scale).astype(BF16)
        accq[c2] = qw

    mst[...] = jnp.full(mst.shape, -jnp.inf, F32)
    nkeys = 2 * ny * sl
    keys_all = nz * nkeys

    def pair(i):
        return pl.ds(pl.multiple_of(i * 2 * nkeys, 2 * nkeys), 2 * nkeys)

    def take(i):
        for u in range(2):
            j = 2 * i + u
            zs = zs_of(j)
            done(kbuf.at[zs, other], kdr.at[zs])
            both = kbuf[zs].reshape(2 * ny, sl + sl // 2, 128)
            latk = both[:, :sl, :].reshape(nkeys, 128)
            rp = both[:, sl:, :]
            rk = jnp.concatenate([rp[:, :, 0:64], rp[:, :, 64:128]], axis=1)
            at = pl.ds(pl.multiple_of(j * nkeys, nkeys), nkeys)
            keyb[at, 0:128] = latk
            keyb[at, 128:192] = rk.reshape(nkeys, 64)
            latt[:, at] = jnp.transpose(latk)

    def score(i, dx):
        sc = mm(keyb[pair(i), :], qt[dx])
        sco[dx, pair(i), :] = sc
        mst[dx] = jnp.maximum(mst[dx], jnp.max(sc.reshape(nkeys // 4, 8, 2 * ht), axis=0))

    def prep(i, _):
        take(i)
        score(i, 0)
        return 0

    def sides_of(i, _):
        for dx in sides:
            score(i, dx)
        return 0

    def across_of(i, _):
        for dx in across:
            score(i, dx)
        return 0

    def all_of(i, _):
        take(i)
        for dx in across + sides + [0]:
            score(i, dx)
        return 0

    def wait_queries(dxs):
        for dx in dxs:
            done(qt.at[dx], qrs.at[dx])

    pairs = nz // 2
    seen_p = n_seen // 2
    cut = [min(n_seen + k, nz) for k in (0, 2, 4, 6)]
    bs = [min(k, n_seen) for k in (3, 5, 7)]
    p0, p1 = min(1, seen_p), min(2, seen_p)
    lax.fori_loop(1, bs[0], step_b, 0)
    lax.fori_loop(cut[0], cut[1], step_a, 0)
    lax.fori_loop(0, p0, prep, 0)
    lax.fori_loop(bs[0], bs[1], step_b, 0)
    lax.fori_loop(cut[1], cut[2], step_a, 0)
    lax.fori_loop(bs[1], bs[2], step_b, 0)
    lax.fori_loop(cut[2], cut[3], step_a, 0)
    lax.fori_loop(p0, p1, prep, 0)

    lax.fori_loop(cut[3], nz, step_a, 0)
    to_mate = rc(kvb.at[1], kvb.at[2 * c], hss.at[0], hrs.at[2 * c], s, mate)
    to_mate.start()
    to_side = rc(kvb.at[1], kvb.at[2 * other], hss.at[1], hrs.at[2 * other], side, mate)
    to_side.start()
    lax.fori_loop(bs[2], n_seen, step_b, 0)
    lax.fori_loop(p1, seen_p, prep, 0)
    wait_queries(sides)
    n_two = seen_p // 2
    rest = nz - n_seen - 2 * n_two

    def rest_b(i, _):
        for u in range(2):
            sides_of(2 * i + u, 0)
        for u in range(2 if rest >= 0 else 0):
            step_b(n_seen + 2 * i + u, 0)
        return 0

    def b_all(i, _):
        step_b(n_seen + 2 * n_two + i, 0)
        return all_of(seen_p + i, 0)

    lax.fori_loop(0, n_two, rest_b, 0)
    lax.fori_loop(2 * n_two, seen_p, sides_of, 0)
    wait_queries(across)
    for i in range(seen_p):
        across_of(i, 0)
    lax.fori_loop(0, max(rest, 0), b_all, 0)
    lax.fori_loop(seen_p + max(rest, 0), pairs, all_of, 0)

    part = min(1024, keys_all)

    def weigh(dx):
        peak = jnp.max(mst[dx], axis=0, keepdims=True)
        l8 = jnp.zeros((8, 2 * ht), F32)
        o = jnp.zeros((128, 2 * ht), F32)
        for k in range(keys_all // part):
            p = jnp.exp2(sco[dx, k * part : (k + 1) * part, :] - peak)
            l8 = l8 + jnp.sum(p.reshape(part // 8, 8, 2 * ht), axis=0)
            o = o + mm(latt[:, k * part : (k + 1) * part], p.astype(BF16))
        l = jnp.sum(l8, axis=0, keepdims=True)
        return (o / l).astype(BF16), jnp.broadcast_to(peak + jnp.log(l) * LOG2E, (8, 2 * ht))

    for i, dx in enumerate(across + sides):
        pos[dx], pls[dx] = weigh(dx)
        xo, back = lax.rem(x + dx, nx), nx - dx
        rc(pls.at[dx], plr.at[back], lss.at[i], lrs.at[back], s, xo * 2 + c).start()
        rc(pos.at[dx], por.at[back], pss.at[i], prs.at[back], s, xo * 2 + c).start()
    por[0], plr[0] = weigh(0)

    for i in (0, 2):
        done(kvb.at[i], hrs.at[i])
    done(wdone[8], wrsem.at[8])
    kpos = lax.broadcasted_iota(jnp.int32, (3 * ht, ht), 0)
    qpos = lax.broadcasted_iota(jnp.int32, (3 * ht, ht), 1)
    apart = jnp.abs(qpos + ht - kpos)
    place = kpos + (s * 2 + c - 1) * ht
    inside = (apart <= WINDOW) & (place >= 0) & (place < sp * tok)
    apart = apart.astype(F32)
    for c2 in range(2):
        kw = kvb[:, c2, :, 0:64].reshape(3 * ht, DH)
        vw = kvb[:, c2, :, 64:128].reshape(3 * ht, DH)
        qw = (accq[c2] * scale).astype(BF16)
        for g in range(2):
            head = (x * 2 + c2) * 2 + g
            slope = jnp.exp2(
                jnp.full((1, ht), -8.0 / (2 * tp), F32) * (head + 1).astype(F32)
            )
            sc = mm(kw, qw[:, g * DH : (g + 1) * DH], NT) * DH ** (-0.5) - slope * apart
            sc = jnp.where(inside, sc, -jnp.inf)
            snk = sinkv[c2, 0:1, g * 128 : g * 128 + 128]
            peak = jnp.maximum(jnp.max(sc, axis=0, keepdims=True), snk)
            w = jnp.exp(sc - peak)
            den = jnp.sum(w, axis=0, keepdims=True) + jnp.exp(snk - peak)
            o = mm(vw, w.astype(BF16), TN) / den
            catt[(c2 * 2 + g) * DH : (c2 * 2 + g + 1) * DH, :] = o.astype(BF16)

    for copy in local[early + 8 :]:
        copy.wait()
    for i in range(5, 8):
        done(wdone[i], wrsem.at[i])
    for dx in range(1, nx):
        done(plr.at[dx], lrs.at[dx])
        done(por.at[dx], prs.at[dx])
    lse = [plr[xp, 0:1, :] for xp in range(nx)]
    top = functools.reduce(jnp.maximum, lse)
    wts = [jnp.exp2(v - top) for v in lse]
    total = functools.reduce(lambda a, b: a + b, wts)
    mixed = por[0].astype(F32) * wts[0]
    for xp in range(1, nx):
        mixed = mixed + por[xp].astype(F32) * wts[xp]
    mixed = (mixed / total).astype(BF16)
    for h in range(2):
        catt[256 + h * 128 : 256 + (h + 1) * 128, :] = mm(
            vupv[h], mixed[:, h * ht : (h + 1) * ht], TN
        ).astype(BF16)
    cat[...] = jnp.transpose(catt[...])

    def out_block(j):
        cols = pl.ds(pl.multiple_of(j * ft, ft), ft)
        return mm(cat[...], wall[:, cols]).astype(BF16)

    def send_block(d, _):
        j = order(d)
        rss[j] = out_block(j)
        rc(rss.at[j], rsr.at[x, c], rs_s.at[d], rs_r.at[x, c], s, j).start()
        return 0

    lax.fori_loop(0, tp - 1, send_block, 0)
    rsr[x, c] = out_block(t)

    def wait_block(d, _):
        j = order(tp - 2 - d)
        jx, jc = j // 2, lax.rem(j, 2)
        done(rsr.at[jx, jc], rs_r.at[jx, jc])
        return 0

    lax.fori_loop(0, tp - 1, wait_block, 0)
    for c2 in range(2):
        total = rsr[0, c2].astype(F32)
        for xp in range(1, nx):
            total = total + rsr[xp, c2].astype(F32)
        out[c2 * ht : (c2 + 1) * ht, :] = total.astype(BF16)

    def sent(d, _):
        done(kps.at[0], kpssem.at[d])
        done(xb.at[0], xssem.at[d])
        done(rss.at[0], rs_s.at[d])
        return 0

    lax.fori_loop(0, tp - 1, sent, 0)
    for copy in wcopies:
        copy.wait_send()
    for i in range(len(near) + len(fwd_up) + len(fwd_down)):
        done(kbuf.at[0, 0, 0], kzs.at[i])

    def sent_keys(zs, _):
        for dy in range(ny - 1):
            done(kbuf.at[0, 0, 0], kys.at[zs, dy])
        done(kbuf.at[0, 0], kds.at[zs])
        return 0

    lax.fori_loop(0, nz, sent_keys, 0)
    for i in range(nx - 1):
        done(qt.at[0], qss.at[i])
        done(pls.at[0], lss.at[i])
        done(pos.at[0], pss.at[i])
    to_mate.wait_send()
    to_side.wait_send()


def tables(sp, tok):
    freq = 1.0 / ROPE_BASE ** (np.arange(0, D_ROPE, 2, dtype=np.float64) / D_ROPE)

    def table(places):
        angle = places[:, None] * freq[None, :]
        flat = np.concatenate([np.cos(angle), np.sin(angle)], axis=1)
        return np.pad(flat, ((0, 0), (0, 64))).astype(np.float32)

    return table(np.arange(sp) * float(tok)), table(np.arange(tok) * 1.0)


def per_device(nz, *args):
    (act, gain, wq, wk, wv, sink, wlq, wkvd, wrope, lgain, kup, vup, ow, ol) = args
    tp, sp = lax.axis_size("tp"), lax.axis_size("sp")
    nx = tp // 2
    ny = sp // nz
    tok, ft = act.shape
    model = tp * ft
    ht, sl = tok // 2, tok // tp
    ta, tb = tables(sp, tok)
    cfg = (nz, ny, nx, tok, ft, model)
    near, up, down = z_plan(nz)
    n_z = len(near) + len(up) + len(down)
    dma = pltpu.SemaphoreType.DMA
    v = pltpu.VMEM
    scratch = [
        v((tok, ft), BF16), v((tp, ft), F32), v((1, 128), F32), v((sp, 128), F32),
        v((tok, 128), F32), pltpu.SMEM((2,), F32), v((2, 8, 256), F32), v((2, model, 128), BF16),
        v((2, 320, model), BF16), v((ft, 128), BF16), v((64, ft), BF16),
        v((2, 128, 128), BF16), v((2, 128, 128), BF16), v((512, model), BF16),
        v((tp, sl, 256), BF16), v((tp, sl, 256), BF16), v((tp, ht, ft), BF16),
        v((2, ht, 128), F32), v((2, ht, 192), F32), v((ht, 1), F32),
        v((nz, 2, ny, sl + sl // 2, 128), BF16), v((nx, 192, 2 * ht), BF16),
        v((3, 2, ht, 128), BF16), v((512, ht), BF16), v((ht, 512), BF16),
        v((nx, tok * sp // nx, 2 * ht), F32),
        v((128, tok * sp // nx), BF16), v((tok * sp // nx, 192), BF16),
        v((nx, 8, 2 * ht), F32),
        v((nx, 128, 2 * ht), BF16), v((nx, 128, 2 * ht), BF16),
        v((nx, 8, 2 * ht), F32), v((nx, 8, 2 * ht), F32),
        v((tp, ht, ft), BF16), v((nx, 2, ht, ft), BF16),
        dma((15 + tp,)), dma((9,)), dma((9,)), dma((tp,)), dma((tp,)), dma((tp,)), dma((tp,)),
        dma((n_z,)), dma((nz,)), dma((nz, max(ny - 1, 1))), dma((nz,)), dma((nz,)), dma((nz,)),
        dma((nx,)), dma((nx,)), dma((2,)), dma((3,)), dma((nx,)), dma((nx,)), dma((nx,)), dma((nx,)),
        dma((tp,)), dma((nx, 2)),
    ]
    keep = lambda a: pltpu.with_memory_space_constraint(a, pltpu.HBM)
    hbm = pl.BlockSpec(memory_space=pltpu.HBM)
    specs = [hbm] * 16
    return pl.pallas_call(
        functools.partial(kernel, cfg),
        out_shape=jax.ShapeDtypeStruct((tok, ft), BF16),
        in_specs=specs,
        out_specs=pl.BlockSpec(memory_space=pltpu.VMEM),
        scratch_shapes=scratch,
        compiler_params=pltpu.CompilerParams(
            collective_id=0, has_side_effects=True, vmem_limit_bytes=44000 * 1024
        ),
    )(
        *map(
            keep,
            (
                act, gain, wq, wk.T, wv.T, sink, wlq.T, wkvd, wrope.T, lgain.reshape(1, 128),
                kup, vup, ow, ol, jnp.asarray(ta), jnp.asarray(tb),
            ),
        )
    )


def solution(mesh):
    return jax.shard_map(
        functools.partial(per_device, mesh.shape["sp"] // NY),
        mesh=mesh,
        in_specs=(
            P("sp", "tp"), P(), P(None, "tp"), P(None, "tp"), P(None, "tp"), P("tp"),
            P(None, "tp"), P(), P(), P(), P(None, "tp"), P(None, "tp"), P("tp", None),
            P("tp", None),
        ),
        out_specs=P("sp", "tp"),
        check_vma=False,
    )
```
